128 devices in a mesh: ep: 64 (over z, y, x), tp: 2 (over core).
Axes of the slice: x: 4, y: 4, z: 4, core: 2. Of those that a mesh axis runs over, the one named last changes fastest.
Arguments:
- tokens: bfloat16 [4096, 2048], P('ep', 'tp'), may hold values from -6 to 6
- sequence_state_real: float32 [4096, 128, 64], P('ep', 'tp'), may hold values from -4 to 4
- sequence_state_imaginary: float32 [4096, 128, 64], P('ep', 'tp'), may hold values from -4 to 4
- mixer_norm_gain: float32 [2048], replicated, may hold values from 0.1 to 1.9
- expert_norm_gain: float32 [2048], replicated, may hold values from 0.1 to 1.9
- rate: float32 [128, 64], P('tp'), may hold values from 0.1 to 4
- freq: float32 [128, 64], P('tp'), may hold values from -3 to 3
- log_group_step: float32 [128], P('tp'), may hold values from -3 to 0
- input_map_real: float32 [128, 64, 16], P('tp'), may hold values from -1 to 1
- input_map_imaginary: float32 [128, 64, 16], P('tp'), may hold values from -1 to 1
- output_map_real: float32 [128, 16, 64], P('tp'), may hold values from -0.75 to 0.75
- output_map_imaginary: float32 [128, 16, 64], P('tp'), may hold values from -0.75 to 0.75
- skip: float32 [2048], P('tp'), may hold values from -4 to 4
- mixer_value_weight: bfloat16 [2048, 2048], P('tp'), may hold values from -0.125 to 0.125
- mixer_gate_weight: bfloat16 [2048, 2048], P('tp'), may hold values from -0.125 to 0.125
- group_router_weight: bfloat16 [2048, 4], replicated, may hold values from -0.125 to 0.125
- expert_router_weight: bfloat16 [2048, 64], replicated, may hold values from -0.125 to 0.125
- dense_blend_weight: float32 [2048], replicated, may hold values from -0.125 to 0.125
- routes: int32 [4096, 2], P('ep'), may hold values from 0 to 63, all different within a row; in each aligned block of 64 rows (0 to 63, 64 to 127, ...) at most 4 rows name the same one
- expert_gate_weight: bfloat16 [64, 2048, 1024], P('ep', None, 'tp'), may hold values from -0.125 to 0.125
- expert_up_weight: bfloat16 [64, 2048, 1024], P('ep', None, 'tp'), may hold values from -0.125 to 0.125
- expert_down_weight: bfloat16 [64, 1024, 2048], P('ep', 'tp'), may hold values from -0.1875 to 0.1875
- shared_gate_weight: bfloat16 [2048, 2048], P('tp', 'ep'), may hold values from -0.125 to 0.125
- shared_up_weight: bfloat16 [2048, 2048], P('tp', 'ep'), may hold values from -0.125 to 0.125
- shared_down_weight: bfloat16 [2048, 2048], P(None, 'tp'), may hold values from -0.125 to 0.125
Outputs:
- result: bfloat16 [4096, 2048], P('ep', 'tp')
- next_re: float32 [4096, 128, 64], P('ep', 'tp')
- next_im: float32 [4096, 128, 64], P('ep', 'tp')
The draws below stay inside these ranges and needn't reach their ends.
Inputs may be any that keep to these rules, and one draw needn't show every extreme that they name: `routes`: each row names 2 different experts. Among the rows of one device no expert is named more than 4 times, and in every draw some expert is named exactly 4 times by some device's rows.
All inputs are finite; a program needn't handle non-finite values.
Results may differ from the reference program's by a relative error of at most 0.017.
Values may be sent and summed in bfloat16 or wider, within the bound.
A program may use at most 128 MiB of HBM per device.

```python
import math
import jax
import jax.numpy as jnp
import numpy as np
from jax import lax

MODEL_WIDTH = 2048
CH = 16
G = 128
P_SIZE = 64
SEQ_DEV = 64
TOKENS = 4096
NG = 4
EXPERT_COUNT = 64
EXPERT_HIDDEN = 1024
FS = 2048
TOPK = 2
CAP = 4
N_EP = 64


def block_levels(key, shape, cuts, least, top_value):
    factor_of, own = 1.0, jax.random.fold_in(key, 6)
    for axis_at, shards_of in cuts:
        steps = jnp.exp(jax.random.uniform(jax.random.fold_in(own, axis_at), (shards_of,), jnp.float32, least / len(cuts), top_value / len(cuts)))
        factor_of = factor_of * jnp.repeat(steps, shape[axis_at] // shards_of).reshape([-1 if axis == axis_at else 1 for axis in range(len(shape))])
    return factor_of


def assign_block(key, own, number, rows, number_of, top, reach, lean):
    sequence = jax.random.permutation(key, number_of)
    crowded, common = load_shares(number_of, rows * top, reach, lean, True), load_shares(number_of, rows * top, reach, lean, False)
    places = jnp.arange(number_of)

    def named(tallies, turn):
        used = int((tallies > 0).sum())
        fixed = max(1, used // 4)
        passed = fixed + (places - fixed + turn * (used - fixed)) % max(1, number_of - fixed)
        return jnp.zeros((number_of,), jnp.int32).at[sequence[jnp.where(places < fixed, places, passed)]].set(jnp.asarray(tallies, jnp.int32))

    tallies = jnp.where(number % 4 == 0, named(crowded, number // 4), named(common, number - number // 4 - 1))
    mixed = jax.random.permutation(jax.random.fold_in(own, 3), number_of)
    donor, sink = mixed[0:number_of // 2 * 2:2], mixed[1:number_of // 2 * 2:2]
    room = jnp.minimum(tallies[donor] - 1, reach - tallies[sink]) // 2
    room = jnp.where((donor == sequence[0]) | (sink == sequence[0]) | (tallies[sink] == 0), 0, jnp.maximum(room, 0))
    passed = jax.random.randint(jax.random.fold_in(own, 4), (number_of // 2,), 0, 1 << 20) % (room + 1)
    tallies = tallies.at[donor].add(-passed).at[sink].add(passed)
    items = jnp.searchsorted(jnp.cumsum(tallies), jnp.arange(rows * top), side="right").astype(jnp.int32)
    table = items.reshape(top, rows).T
    table = table[jax.random.permutation(jax.random.fold_in(own, 1), rows)]
    turn = jax.random.randint(jax.random.fold_in(own, 2), (rows, 1), 0, top)
    return jnp.take_along_axis(table, (jnp.arange(top)[None, :] + turn) % top, axis=1)


def load_shares(amount, total, bound, slope, full):
    loads = [(1 << 20) // math.isqrt(rank ** slope) + 1 for rank in range(1, amount + 1)]
    largest = bound if full else min(bound, max(-(-total // amount), total * loads[0] // sum(loads)))
    least = 1 if total - largest >= amount - 1 else 0
    given, surplus = [largest] + [least] * (amount - 1), total - largest - least * (amount - 1)
    while surplus > 0:
        free = [i for i in range(1, amount) if given[i] < largest] or [i for i in range(1, amount) if given[i] < bound]
        pool, remaining = sum([loads[i] for i in free]), surplus
        for i in free:
            more = min(bound - given[i], max(1, remaining * loads[i] // pool), surplus)
            given[i] = given[i] + more
            surplus = surplus - more
    return np.array(given)


def scatter_about(key, extent, deviation, most, cuts=(), kind=jnp.bfloat16):
    values = jax.random.normal(key, extent, jnp.float32) * deviation
    if len(cuts) > 0:
        values = block_levels(key, extent, cuts, -0.22, 0.18) * values
    return jnp.clip(values, min=-most, max=most).astype(kind)


def setup_inputs(seed: int = 0) -> dict:
    key_list = jax.random.split(jax.random.key(seed), 26)
    tokens = scatter_about(key_list[0], (TOKENS, MODEL_WIDTH), 1.0, 6.0, ((0, 64), (1, 2)))
    sequence_state_real = scatter_about(key_list[1], (TOKENS, G, P_SIZE), 0.5, 4.0, ((0, 64), (1, 2)), jnp.float32)
    sequence_state_imaginary = scatter_about(key_list[2], (TOKENS, G, P_SIZE), 0.5, 4.0, ((0, 64), (1, 2)), jnp.float32)
    mixer_norm_gain = jnp.clip(1.0 + 0.18 * jax.random.normal(key_list[3], (MODEL_WIDTH,), jnp.float32), 0.1, 1.9)
    expert_norm_gain = jnp.clip(1.0 + 0.18 * jax.random.normal(key_list[4], (MODEL_WIDTH,), jnp.float32), 0.1, 1.9)
    rate = jnp.clip(jnp.exp(math.log(4.0) - 3.6888794 * jax.random.uniform(key_list[5], (G, P_SIZE), jnp.float32) ** block_levels(key_list[5], (G, P_SIZE), ((0, 2),), -0.2, 0.2)), 0.1, 4.0)
    freq = jnp.clip(jax.random.uniform(key_list[6], (G, P_SIZE), jnp.float32, -3.0, 3.0) * block_levels(key_list[6], (G, P_SIZE), ((0, 2),), -0.4, 0.0), -3.0, 3.0)
    log_group_step = jnp.clip(-3.0 + 3.0 * jax.random.uniform(key_list[7], (G,), jnp.float32) ** block_levels(key_list[7], (G,), ((0, 2),), -0.2, 0.2), -3.0, 0.0)
    input_map_real = scatter_about(key_list[8], (G, P_SIZE, CH), (2 * CH) ** -0.5, 1.0, ((0, 2),), jnp.float32)
    input_map_imaginary = scatter_about(key_list[9], (G, P_SIZE, CH), (2 * CH) ** -0.5, 1.0, ((0, 2),), jnp.float32)
    output_map_real = scatter_about(key_list[10], (G, CH, P_SIZE), P_SIZE ** -0.5, 0.75, ((0, 2),), jnp.float32)
    output_map_imaginary = scatter_about(key_list[11], (G, CH, P_SIZE), P_SIZE ** -0.5, 0.75, ((0, 2),), jnp.float32)
    skip = scatter_about(key_list[12], (MODEL_WIDTH,), 1.0, 4.0, ((0, 2),), jnp.float32)
    mixer_value_weight = scatter_about(key_list[13], (MODEL_WIDTH, MODEL_WIDTH), MODEL_WIDTH ** -0.5, 0.125, ((0, 2),))
    mixer_gate_weight = scatter_about(key_list[14], (MODEL_WIDTH, MODEL_WIDTH), MODEL_WIDTH ** -0.5, 0.125, ((0, 2),))
    group_router_weight = scatter_about(key_list[15], (MODEL_WIDTH, NG), MODEL_WIDTH ** -0.5, 0.125)
    expert_router_weight = scatter_about(key_list[16], (MODEL_WIDTH, EXPERT_COUNT), MODEL_WIDTH ** -0.5, 0.125)
    dense_blend_weight = scatter_about(key_list[17], (MODEL_WIDTH,), MODEL_WIDTH ** -0.5, 0.125, (), jnp.float32)
    routes_keys = jax.random.split(jax.random.fold_in(key_list[18], 1), TOKENS // SEQ_DEV)
    routes_turns = jax.random.permutation(jax.random.fold_in(key_list[18], 3), TOKENS // SEQ_DEV)
    routes = jax.vmap(lambda own, number: assign_block(jax.random.fold_in(key_list[18], 2), own, number, SEQ_DEV, EXPERT_COUNT, TOPK, CAP, 2))(routes_keys, routes_turns).reshape((TOKENS, TOPK))
    expert_gate_weight = scatter_about(key_list[19], (EXPERT_COUNT, MODEL_WIDTH, EXPERT_HIDDEN), MODEL_WIDTH ** -0.5, 0.125, ((0, 64), (2, 2)))
    expert_up_weight = scatter_about(key_list[20], (EXPERT_COUNT, MODEL_WIDTH, EXPERT_HIDDEN), MODEL_WIDTH ** -0.5, 0.125, ((0, 64), (2, 2)))
    expert_down_weight = scatter_about(key_list[21], (EXPERT_COUNT, EXPERT_HIDDEN, MODEL_WIDTH), EXPERT_HIDDEN ** -0.5, 0.1875, ((0, 64), (1, 2)))
    shared_gate_weight = scatter_about(key_list[22], (MODEL_WIDTH, FS), MODEL_WIDTH ** -0.5, 0.125, ((0, 2), (1, 64)))
    shared_up_weight = scatter_about(key_list[23], (MODEL_WIDTH, FS), MODEL_WIDTH ** -0.5, 0.125, ((0, 2), (1, 64)))
    shared_down_weight = scatter_about(key_list[24], (FS, MODEL_WIDTH), FS ** -0.5, 0.125, ((1, 2),))
    return dict(tokens=tokens, sequence_state_real=sequence_state_real, sequence_state_imaginary=sequence_state_imaginary, mixer_norm_gain=mixer_norm_gain, expert_norm_gain=expert_norm_gain, rate=rate, freq=freq, log_group_step=log_group_step, input_map_real=input_map_real, input_map_imaginary=input_map_imaginary, output_map_real=output_map_real, output_map_imaginary=output_map_imaginary, skip=skip, mixer_value_weight=mixer_value_weight, mixer_gate_weight=mixer_gate_weight, group_router_weight=group_router_weight, expert_router_weight=expert_router_weight, dense_blend_weight=dense_blend_weight, routes=routes, expert_gate_weight=expert_gate_weight, expert_up_weight=expert_up_weight, expert_down_weight=expert_down_weight, shared_gate_weight=shared_gate_weight, shared_up_weight=shared_up_weight, shared_down_weight=shared_down_weight)


EPS = 1e-06
PRECISION_MAX = lax.Precision.HIGHEST

def row_scale(values):
    return lax.rsqrt(lax.optimization_barrier(jnp.mean(values * values, axis=-1, keepdims=True)) + EPS)

def narrow(values):
    return lax.optimization_barrier(values.astype(jnp.bfloat16)).astype(jnp.float32)

def split_product(left, right):
    middle = left.shape[1] // 2
    first = jnp.dot(left[:, :middle], right[:middle], preferred_element_type=jnp.float32)
    second = jnp.dot(left[:, middle:], right[middle:], preferred_element_type=jnp.float32)
    return narrow(first) + narrow(second)

def state_factors(rate, freq, log_group_step, input_map_real, input_map_imaginary):
    step_size = jnp.exp(log_group_step)[:, None]
    magnitude = jnp.exp(-rate * step_size)
    abar_re = magnitude * jnp.cos(freq * step_size)
    abar_im = magnitude * jnp.sin(freq * step_size)
    denom = rate * rate + freq * freq
    shift_re = abar_re - 1.0
    fac_re = (abar_im * freq - shift_re * rate) / denom
    fac_im = -(abar_im * rate + shift_re * freq) / denom
    bbar_re = fac_re[:, :, None] * input_map_real - fac_im[:, :, None] * input_map_imaginary
    bbar_im = fac_re[:, :, None] * input_map_imaginary + fac_im[:, :, None] * input_map_real
    return (abar_re, abar_im, bbar_re, bbar_im)

def state_step(normed, sequence_state_real, sequence_state_imaginary, factors, output_map_real, output_map_imaginary, skip):
    abar_re, abar_im, bbar_re, bbar_im = factors
    groups = abar_re.shape[0]
    inputs = normed.astype(jnp.float32)
    grouped = inputs.reshape(inputs.shape[0], groups, -1)
    drive_re = jnp.einsum('tgc,gpc->tgp', grouped, bbar_re, precision=PRECISION_MAX)
    drive_im = jnp.einsum('tgc,gpc->tgp', grouped, bbar_im, precision=PRECISION_MAX)
    fresh_real = abar_re * sequence_state_real - abar_im * sequence_state_imaginary + drive_re
    fresh_imaginary = abar_re * sequence_state_imaginary + abar_im * sequence_state_real + drive_im
    state_readout = jnp.einsum('dor,zdr->zdo', output_map_real, fresh_real, precision=PRECISION_MAX)
    state_readout = state_readout - jnp.einsum('dor,zdr->zdo', output_map_imaginary, fresh_imaginary, precision=PRECISION_MAX)
    mixed = state_readout.reshape(inputs.shape) + skip * inputs
    return (mixed, fresh_real, fresh_imaginary)

def route_weights(group_logits, expert_logits, routes):
    per_group = expert_logits.shape[1] // group_logits.shape[1]
    group_prob = jax.nn.softmax(group_logits, axis=-1)
    chosen = jnp.take_along_axis(expert_logits, routes, axis=1)
    picked_group = jnp.take_along_axis(group_prob, routes // per_group, axis=1)
    return jax.nn.softmax(chosen, axis=1) * picked_group

def reference(tokens, sequence_state_real, sequence_state_imaginary, mixer_norm_gain, expert_norm_gain, rate, freq, log_group_step, input_map_real, input_map_imaginary, output_map_real, output_map_imaginary, skip, mixer_value_weight, mixer_gate_weight, group_router_weight, expert_router_weight, dense_blend_weight, routes, expert_gate_weight, expert_up_weight, expert_down_weight, shared_gate_weight, shared_up_weight, shared_down_weight):
    float_tokens = tokens.astype(jnp.float32)
    normed = (float_tokens * row_scale(float_tokens) * mixer_norm_gain).astype(jnp.bfloat16)
    factors = state_factors(rate, freq, log_group_step, input_map_real, input_map_imaginary)
    mixed, next_re, next_im = state_step(normed, sequence_state_real, sequence_state_imaginary, factors, output_map_real, output_map_imaginary, skip)
    activated = jax.nn.gelu(mixed).astype(jnp.bfloat16)
    value = split_product(activated, mixer_value_weight)
    gate = split_product(activated, mixer_gate_weight)
    mix = (value * jax.nn.sigmoid(gate)).astype(jnp.bfloat16)
    hidden = (float_tokens + mix.astype(jnp.float32)).astype(jnp.bfloat16)
    hidden_f32 = hidden.astype(jnp.float32)
    inverse = row_scale(hidden_f32)
    scaled = hidden_f32 * expert_norm_gain
    hnorm = (scaled * inverse).astype(jnp.bfloat16)
    group_logits = jnp.dot(scaled, group_router_weight.astype(jnp.float32), precision=PRECISION_MAX) * inverse
    expert_logits = jnp.dot(scaled, expert_router_weight.astype(jnp.float32), precision=PRECISION_MAX) * inverse
    blend_logit = jnp.dot(scaled, dense_blend_weight, precision=PRECISION_MAX) * inverse[:, 0]
    weight = route_weights(group_logits, expert_logits, routes)
    top_count = routes.shape[1]
    width = tokens.shape[1]
    flat_routes = routes.reshape(-1)
    order = jnp.argsort(flat_routes, stable=True).astype(jnp.int32)
    sorted_ids = flat_routes[order]
    expert_ids = jnp.arange(expert_router_weight.shape[1], dtype=jnp.int32)
    starts = jnp.searchsorted(sorted_ids, expert_ids, side='left').astype(jnp.int32)
    ends = jnp.searchsorted(sorted_ids, expert_ids, side='right').astype(jnp.int32)
    limit = N_EP * CAP
    padded = jnp.concatenate([order, jnp.zeros((limit,), jnp.int32)])
    flat_weight = weight.reshape(-1)

    def one_expert(index_value):
        picks = lax.dynamic_slice_in_dim(padded, starts[index_value], limit)
        live = (jnp.arange(limit, dtype=jnp.int32) < ends[index_value] - starts[index_value]).astype(jnp.float32)
        token_rows = hnorm[picks // top_count]
        gate_e = jnp.dot(token_rows, expert_gate_weight[index_value], preferred_element_type=jnp.float32)
        expert_up_rows = jnp.dot(token_rows, expert_up_weight[index_value], preferred_element_type=jnp.float32)
        inner = (jax.nn.silu(gate_e) * expert_up_rows).astype(jnp.bfloat16)
        expert_out = split_product(inner, expert_down_weight[index_value]).astype(jnp.bfloat16).astype(jnp.float32)
        return (expert_out * (flat_weight[picks] * live)[:, None], picks // top_count)
    contrib, targets = lax.map(one_expert, expert_ids)
    routed = jnp.zeros((tokens.shape[0], width), jnp.float32).at[targets.reshape(-1)].add(contrib.reshape(-1, width))
    dense_gate = split_product(hnorm, shared_gate_weight)
    dense_up = split_product(hnorm, shared_up_weight)
    dense_inner = (jax.nn.silu(dense_gate) * dense_up).astype(jnp.bfloat16)
    dense_out = jnp.dot(dense_inner, shared_down_weight, preferred_element_type=jnp.float32)
    result = hidden_f32 + routed + jax.nn.sigmoid(blend_logit)[:, None] * dense_out
    return (result.astype(jnp.bfloat16), next_re, next_im)
```

```python
import jax
import jax.numpy as jnp
from jax import lax
from jax.experimental import pallas as pl
from jax.experimental.pallas import tpu as pltpu
from jax.sharding import PartitionSpec as P

MESH = pl.DeviceIdType.MESH
BF = jnp.bfloat16
F32 = jnp.float32
I32 = jnp.int32
EPS = 1e-06
NEP = 64
ROWS = 64
HALF = 1024
WIDTH = 2048
PITCH = 72
REACH = ((1, 0, 0), (3, 0, 0), (0, 1, 0), (0, 3, 0), (0, 0, 1), (1, 3, 0), (1, 1, 0))


def nn(a, b):
    return jnp.dot(a, b, preferred_element_type=F32)


def nt(a, b):
    return lax.dot_general(a, b, (((1,), (1,)), ((), ())), preferred_element_type=F32)


def iota(shape, dim):
    return lax.broadcasted_iota(I32, shape, dim)


def onehot(condition):
    return jnp.where(condition, 1.0, 0.0).astype(BF)


def column(row, n):
    spread = jnp.where(iota((n, n), 0) == iota((n, n), 1), jnp.broadcast_to(row, (n, n)), 0.0)
    return jnp.sum(spread, axis=1, keepdims=True)


def sigmoid(x):
    return 1.0 / (1.0 + jnp.exp(-x))


def gelu(x):
    return x * (0.5 * (1.0 + jnp.tanh(0.7978845608028654 * (x + 0.044715 * (x * x * x)))))


def shard_of(colour, member):
    z = member % 4
    y = 2 * (member // 4) + colour % 2
    x = (colour // 2 + 16 - y - 2 * z) % 4
    return z * 16 + y * 4 + x


def body(
    tok, mgain, egain, rate, freq, lgs, skip, grw, erw, blend, routes,
    sre, sim, imr, imi, omr, omi, wv, wg, eg, eu, ed, sg, su, sd,
    out, nre, nim,
    sre_v, sim_v, imr_v, imi_v, omr_v, omi_v, wv_v, wg_v, eg_v, eu_v, ed_v, sd_v, wbg, wbu,
    fre, fim, are, aim, bre, bim, cre, cim, vbuf, abuf, rt, dmat, dtmat, m0s, m1s, perm, permt,
    e1s, e1r, vgs, vgr, e3s, e3r, dsend, xo, xp, xx, acc, inner, pts, ptr, ptot, rsend, ret,
    tb, dps, dpr, dis, dn, hid,
    lsem, e_send, e_recv, w_send, w_recv, d_send, d_recv, t_send, t_recv, r_send, r_recv, n_send, n_recv,
):
    ep = lax.axis_index("ep")
    tp = lax.axis_index("tp")
    other = 1 - tp
    x = ep % 4
    y = (ep // 4) % 4
    z = ep // 16
    colour = 2 * ((x + y + 2 * z) % 4) + y % 2
    member = (y // 2) * 4 + z
    own_cols = pl.ds(pl.multiple_of(tp * HALF, HALF), HALF)
    peer_cols = pl.ds(pl.multiple_of(other * HALF, HALF), HALF)

    barrier = pltpu.get_barrier_semaphore()
    me = ep * 2 + tp

    def greet(i, carry):
        d = (me + 1 + i) % (2 * NEP)
        pl.semaphore_signal(barrier, inc=1, device_id=(d // 2, d % 2), device_id_type=MESH)
        return carry

    lax.fori_loop(0, 2 * NEP - 1, greet, 0)

    def load(src, dst, k):
        c = pltpu.make_async_copy(src, dst, lsem.at[k])
        c.start()
        return c

    l_imr = load(imr, imr_v, 0)
    l_imi = load(imi, imi_v, 1)

    def load_state(t, carry):
        rows = pl.ds(pl.multiple_of(t * PITCH, 8), 64)
        pltpu.make_async_copy(sre.at[t], sre_v.at[rows], lsem.at[2]).start()
        pltpu.make_async_copy(sim.at[t], sim_v.at[rows], lsem.at[3]).start()
        return carry

    lax.fori_loop(0, ROWS, load_state, 0)
    l_omr = load(omr, omr_v, 4)
    l_omi = load(omi, omi_v, 5)
    l_wv1 = load(wv.at[:, peer_cols], wv_v.at[0], 6)
    l_wg1 = load(wg.at[:, peer_cols], wg_v.at[0], 7)
    l_wv0 = load(wv.at[:, own_cols], wv_v.at[1], 8)
    l_wg0 = load(wg.at[:, own_cols], wg_v.at[1], 9)
    l_eg = load(eg.at[0], eg_v, 10)
    l_eu = load(eu.at[0], eu_v, 11)
    l_ed = load(ed.at[0], ed_v, 12)
    wslot = pl.ds(pl.multiple_of(member * 32, 32), 32)
    l_sg = load(sg, wbg.at[wslot], 13)
    l_su = load(su, wbu.at[wslot], 14)

    def load_down(p, carry):
        i = shard_of(p // 8, p % 8)
        pltpu.make_async_copy(
            sd.at[pl.ds(pl.multiple_of(i * 32, 32), 32)], sd_v.at[pl.ds(pl.multiple_of(p * 32, 32), 32)], lsem.at[15]
        ).start()
        return carry

    lax.fori_loop(0, 64, load_down, 0)

    tokf = tok[...].astype(F32)
    ss = jnp.sum(tokf * tokf, axis=1, keepdims=True)
    e1s[...] = jnp.broadcast_to(ss, (ROWS, 128))

    step = jnp.exp(column(lgs[...], 64))
    mag = jnp.exp(-rate[...] * step)
    a_re = mag * jnp.cos(freq[...] * step)
    a_im = mag * jnp.sin(freq[...] * step)
    denom = rate[...] * rate[...] + freq[...] * freq[...]
    sh_re = a_re - 1.0
    fre[...] = (a_im * freq[...] - sh_re * rate[...]) / denom
    fim[...] = -(a_im * rate[...] + sh_re * freq[...]) / denom
    are[...] = a_re
    aim[...] = a_im
    l_imr.wait()
    l_imi.wait()

    def make_b(g, carry):
        rows = pl.ds(pl.multiple_of(g * 16, 16), 16)
        f_re = fre[pl.ds(g, 1), :]
        f_im = fim[pl.ds(g, 1), :]
        m_re = imr_v[rows, :]
        m_im = imi_v[rows, :]
        bre[rows, :] = (f_re * m_re - f_im * m_im).astype(BF)
        bim[rows, :] = (f_re * m_im + f_im * m_re).astype(BF)
        return carry

    lax.fori_loop(0, 64, make_b, 0)

    pl.semaphore_wait(barrier, 2 * NEP - 1)

    def exchange(src, dst, k):
        c = pltpu.make_async_remote_copy(
            src_ref=src, dst_ref=dst, send_sem=e_send.at[k], recv_sem=e_recv.at[k],
            device_id=(ep, other), device_id_type=MESH,
        )
        c.start()
        return c

    x1 = exchange(e1s, e1r, 0)

    def send_weights(k, carry):
        dest = shard_of(colour, (member + k) % 8)
        pltpu.make_async_remote_copy(
            src_ref=sg, dst_ref=wbg.at[wslot], send_sem=w_send.at[0], recv_sem=w_recv.at[0],
            device_id=(dest, tp), device_id_type=MESH,
        ).start()
        pltpu.make_async_remote_copy(
            src_ref=su, dst_ref=wbu.at[wslot], send_sem=w_send.at[1], recv_sem=w_recv.at[1],
            device_id=(dest, tp), device_id_type=MESH,
        ).start()
        return carry

    lax.fori_loop(1, 8, send_weights, 0)

    r0 = routes[0:1, :].astype(F32)
    r1 = routes[1:2, :].astype(F32)
    e_sub = iota((64, 64), 0).astype(F32)
    e_lane = iota((64, 64), 1).astype(F32)
    m0 = onehot(e_sub == r0)
    m1 = onehot(e_sub == r1)
    sub4 = iota((64, 256), 0)
    lane4 = iota((64, 256), 1) % 64
    same4 = onehot(sub4 == lane4)
    before4 = onehot(sub4 < lane4)
    n0 = jnp.sum(m0.astype(F32), axis=1, keepdims=True)
    a4 = nn(m0, same4) * (nn(m0, before4) + 1.0) + nn(m1, same4) * (nn(m1, before4) + n0 + 1.0)
    a4 = a4.astype(BF)

    def make_d(q, carry):
        row = iota((256, 1), 0)
        spread = onehot((row // 16 + q * 16) == iota((256, 64), 1))
        got = nn(spread, a4)
        hit = (got == ((row % 4) + 1).astype(F32)) & (((row // 4) % 4) == (iota((256, 256), 1) // 64))
        dmat[pl.ds(pl.multiple_of(q * 256, 256), 256), :] = onehot(hit)
        return carry

    lax.fori_loop(0, 4, make_d, 0)

    c0 = column(r0, 64)
    c1 = column(r1, 64)
    t0 = onehot(e_lane == c0)
    t1 = onehot(e_lane == c1)
    earlier = onehot(iota((64, 64), 1) < iota((64, 64), 0))
    b0 = (t0.astype(F32) * (nn(earlier, t0) + 1.0)).astype(BF)
    b1 = (t1.astype(F32) * (nn(earlier, t1) + jnp.sum(t0.astype(F32), axis=0, keepdims=True) + 1.0)).astype(BF)
    m0s[...] = t0.astype(F32)
    m1s[...] = t1.astype(F32)

    def make_dt(q, carry):
        lane = iota((1, 256), 1)
        spread = onehot((iota((64, 256), 0)) == (iota((64, 256), 1) // 16 + q * 16))
        want = ((lane % 4) + 1).astype(F32)
        cols = pl.ds(pl.multiple_of(q * 256, 256), 256)
        for route, coded in enumerate((b0, b1)):
            got = nn(coded, spread) == want
            for k in range(4):
                rows = pl.ds(route * 256 + k * 64, 64)
                dtmat[rows, cols] = onehot(got & (((lane // 4) % 4) == k))
        return carry

    lax.fori_loop(0, 4, make_dt, 0)
    pi = iota((256, 256), 0)
    pj = iota((256, 256), 1)
    perm[...] = onehot((((pi // 4) % 16) * 16 + (pi // 64) * 4 + pi % 4) == pj)
    permt[...] = onehot((((pi // 4) % 4) * 64 + (pi // 16) * 4 + pi % 4) == pj)
    rt[0:64, :] = erw[:, own_cols]
    rt[64:128, :] = jnp.concatenate([grw[:, own_cols].astype(F32), jnp.zeros((60, HALF), F32)], axis=0).astype(BF)

    x1.wait()
    total = ss + e1r[:, 0:1]
    scale = lax.rsqrt(total / WIDTH + EPS)
    vbuf[...] = (tokf * scale * mgain[:, own_cols]).astype(BF)
    l_omr.wait()
    l_omi.wait()
    cre[...] = omr_v[...].astype(BF)
    cim[...] = omi_v[...].astype(BF)
    pltpu.make_async_copy(sre, sre, lsem.at[2]).wait()
    pltpu.make_async_copy(sim, sim, lsem.at[3]).wait()
    lane_group = iota((ROWS, 128), 1) // 16

    def state_block(b, carry):
        cols = pl.ds(pl.multiple_of(b * 128, 128), 128)
        u = vbuf[:, cols]
        spread = jnp.concatenate([jnp.where(lane_group == j, u, jnp.zeros_like(u)) for j in range(8)], axis=0)
        d_re = nn(spread, bre[cols, :])
        d_im = nn(spread, bim[cols, :])
        fresh_re = []
        fresh_im = []
        for j in range(8):
            g = b * 8 + j
            at = pl.ds(g, ROWS, stride=PITCH)
            s_re = sre_v[at, :]
            s_im = sim_v[at, :]
            g_re = are[pl.ds(g, 1), :]
            g_im = aim[pl.ds(g, 1), :]
            n_re = g_re * s_re - g_im * s_im + d_re[j * ROWS:(j + 1) * ROWS]
            n_im = g_re * s_im + g_im * s_re + d_im[j * ROWS:(j + 1) * ROWS]
            sre_v[at, :] = n_re
            sim_v[at, :] = n_im
            fresh_re.append(n_re.astype(BF))
            fresh_im.append(n_im.astype(BF))
        read = nt(jnp.concatenate(fresh_re, axis=0), cre[cols, :]) - nt(jnp.concatenate(fresh_im, axis=0), cim[cols, :])
        mixed = skip[:, cols] * u.astype(F32)
        for j in range(8):
            mixed = mixed + jnp.where(lane_group == j, read[j * ROWS:(j + 1) * ROWS], 0.0)
        abuf[:, cols] = gelu(mixed).astype(BF)
        return carry

    lax.fori_loop(0, 8, state_block, 0)

    def store_state(t, carry):
        rows = pl.ds(pl.multiple_of(t * PITCH, 8), 64)
        pltpu.make_async_copy(sre_v.at[rows], nre.at[t], lsem.at[16]).start()
        pltpu.make_async_copy(sim_v.at[rows], nim.at[t], lsem.at[17]).start()
        return carry

    lax.fori_loop(0, ROWS, store_state, 0)

    act = abuf[...]
    l_wv1.wait()
    vgs[0] = nn(act, wv_v[0]).astype(BF)
    x2 = exchange(vgs.at[0], vgr.at[0], 1)
    l_wg1.wait()
    vgs[1] = nn(act, wg_v[0]).astype(BF)
    x3 = exchange(vgs.at[1], vgr.at[1], 2)
    l_wv0.wait()
    value = nn(act, wv_v[1]).astype(BF).astype(F32)
    l_wg0.wait()
    gate = nn(act, wg_v[1]).astype(BF).astype(F32)
    x2.wait()
    x3.wait()
    value = value + vgr[0].astype(F32)
    gate = gate + vgr[1].astype(F32)
    mix = (value * sigmoid(gate)).astype(BF)
    hidden = (tok[...].astype(F32) + mix.astype(F32)).astype(BF).astype(F32)
    hid[...] = hidden
    scaled = hidden * egain[:, own_cols]
    top = scaled.astype(BF)
    rest = (scaled - top.astype(F32)).astype(BF)
    logits = nt(top, rt[...]) + nt(rest, rt[...])
    blend_part = jnp.sum(scaled * blend[:, own_cols], axis=1, keepdims=True)
    square_part = jnp.sum(hidden * hidden, axis=1, keepdims=True)
    lane = iota((ROWS, 128), 1)
    logits = jnp.where(lane == 68, blend_part, jnp.where(lane == 69, square_part, logits))
    e3s[...] = logits
    x4 = exchange(e3s, e3r, 3)
    x4.wait()
    logits = logits + e3r[...]
    squares = jnp.sum(jnp.where(lane == 69, logits, 0.0), axis=1, keepdims=True)
    inverse = lax.rsqrt(squares / WIDTH + EPS)
    hnorm = (scaled * inverse).astype(BF)
    logits = logits * inverse

    tb[0:ROWS, :] = hnorm
    quarters = jnp.concatenate([hnorm[:, k * 256:(k + 1) * 256] for k in range(4)], axis=0)
    dsend[...] = nn(dmat[...], quarters).astype(BF)
    mine = pl.ds(pl.multiple_of(ep * 16, 16), 16)
    xo[mine, :] = dsend[mine, :]

    def send_rows(src, dst, ssem, rsem):
        def go(d, carry):
            dest = ((z + d // 16) % 4) * 16 + ((y + (d // 4) % 4) % 4) * 4 + (x + d % 4) % 4
            pltpu.make_async_remote_copy(
                src_ref=src.at[pl.ds(pl.multiple_of(dest * 16, 16), 16)], dst_ref=dst.at[mine],
                send_sem=ssem, recv_sem=rsem, device_id=(dest, tp), device_id_type=MESH,
            ).start()
            return carry

        lax.fori_loop(1, NEP, go, 0)

    send_rows(dsend, xo, d_send, d_recv)
    tok_copies = []
    for i, (dx, dy, dz) in enumerate(REACH):
        dest = ((z + dz) % 4) * 16 + ((y + dy) % 4) * 4 + (x + dx) % 4
        c = pltpu.make_async_remote_copy(
            src_ref=tb.at[pl.ds(0, ROWS)], dst_ref=tb.at[pl.ds((i + 1) * ROWS, ROWS)],
            send_sem=t_send.at[i], recv_sem=t_recv.at[i], device_id=(dest, tp), device_id_type=MESH,
        )
        c.start()
        tok_copies.append(c)

    blend_logit = jnp.sum(jnp.where(lane == 68, logits, 0.0), axis=1, keepdims=True)
    is_group = (lane >= 64) & (lane < 68)
    group_max = jnp.max(jnp.where(is_group, logits, -jnp.inf), axis=1, keepdims=True)
    group_exp = jnp.where(is_group, jnp.exp(jnp.where(is_group, logits, group_max) - group_max), 0.0)
    group_prob = group_exp / jnp.sum(group_exp, axis=1, keepdims=True)
    row0 = column(routes[0:1, :].astype(F32), 64).astype(I32)
    row1 = column(routes[1:2, :].astype(F32), 64).astype(I32)
    pick0 = jnp.sum(jnp.where(lane == row0, logits, 0.0), axis=1, keepdims=True)
    pick1 = jnp.sum(jnp.where(lane == row1, logits, 0.0), axis=1, keepdims=True)
    prob0 = jnp.sum(jnp.where(lane == 64 + row0 // 16, group_prob, 0.0), axis=1, keepdims=True)
    prob1 = jnp.sum(jnp.where(lane == 64 + row1 // 16, group_prob, 0.0), axis=1, keepdims=True)
    top_pick = jnp.maximum(pick0, pick1)
    exp0 = jnp.exp(pick0 - top_pick)
    exp1 = jnp.exp(pick1 - top_pick)
    weight0 = exp0 / (exp0 + exp1) * prob0
    weight1 = exp1 / (exp0 + exp1) * prob1
    blend_gate = sigmoid(blend_logit)

    bulk = pl.ds(0, (NEP - 1) * 16)
    pltpu.make_async_copy(xo.at[bulk], xo.at[bulk], d_recv).wait()
    x5 = exchange(xo, xp, 4)
    l_eg.wait()
    l_eu.wait()

    def unpack(src):
        for q in range(4):
            got = nn(perm[...], src[q * 256:(q + 1) * 256, :]).astype(BF)
            for k in range(4):
                xx[q * 64:(q + 1) * 64, k * 256:(k + 1) * 256] = got[k * 64:(k + 1) * 64]

    unpack(xo)
    acc[0] = nn(xx[...], eg_v[own_cols, :])
    acc[1] = nn(xx[...], eu_v[own_cols, :])
    x5.wait()
    unpack(xp)
    gate_e = acc[0] + nn(xx[...], eg_v[peer_cols, :])
    up_e = acc[1] + nn(xx[...], eu_v[peer_cols, :])
    inner[...] = (gate_e * sigmoid(gate_e) * up_e).astype(BF)
    l_ed.wait()
    pts[...] = nn(inner[...], ed_v[:, peer_cols]).astype(BF)
    x6 = exchange(pts, ptr, 5)
    part = nn(inner[...], ed_v[:, own_cols]).astype(BF)
    ptot[...] = part
    x6.wait()
    ptot[...] = (ptot[...].astype(F32) + ptr[...].astype(F32)).astype(BF)
    for q in range(4):
        rows = slice(q * 64, (q + 1) * 64)
        block = jnp.concatenate([ptot[rows, k * 256:(k + 1) * 256] for k in range(4)], axis=0)
        rsend[q * 256:(q + 1) * 256, :] = nn(permt[...], block).astype(BF)
    ret[mine, :] = rsend[mine, :]
    send_rows(rsend, ret, r_send, r_recv)

    l_sg.wait()
    l_su.wait()
    most = pl.ds(0, 7 * 32)
    pltpu.make_async_copy(wbg.at[most], wbg.at[most], w_recv.at[0]).wait()
    pltpu.make_async_copy(wbu.at[most], wbu.at[most], w_recv.at[1]).wait()
    for c in tok_copies:
        c.wait()
    peer_units = pl.ds(pl.multiple_of(other * 128, 128), 128)
    own_units = pl.ds(pl.multiple_of(tp * 128, 128), 128)
    dps[0] = nt(tb[...], wbg[peer_units, :]).astype(BF)
    dps[1] = nt(tb[...], wbu[peer_units, :]).astype(BF)
    x7 = exchange(dps, dpr, 6)
    dgate = nt(tb[...], wbg[own_units, :]).astype(BF).astype(F32)
    dup = nt(tb[...], wbu[own_units, :]).astype(BF).astype(F32)
    x7.wait()
    dgate = dgate + dpr[0].astype(F32)
    dup = dup + dpr[1].astype(F32)
    dis[...] = (dgate * sigmoid(dgate) * dup).astype(BF)
    slot = pl.ds(pl.multiple_of((colour * 2 + tp) * ROWS, ROWS), ROWS)
    dn[slot, :] = dis[0:ROWS, :]

    def send_inner(i, dest, core):
        pltpu.make_async_remote_copy(
            src_ref=dis.at[pl.ds(i * ROWS, ROWS)], dst_ref=dn.at[slot], send_sem=n_send, recv_sem=n_recv,
            device_id=(dest, core), device_id_type=MESH,
        ).start()

    send_inner(0, ep, other)
    for i, (dx, dy, dz) in enumerate(REACH):
        dest = ((z + 4 - dz) % 4) * 16 + ((y + 4 - dy) % 4) * 4 + (x + 4 - dx) % 4
        send_inner(i + 1, dest, tp)
        send_inner(i + 1, dest, other)
    pltpu.make_async_copy(sd, sd, lsem.at[15]).wait()
    fifteen = pl.ds(0, 15 * ROWS)
    pltpu.make_async_copy(dn.at[fifteen], dn.at[fifteen], n_recv).wait()
    dense_inner = jnp.concatenate([dn[s * ROWS:(s + 1) * ROWS, :] for s in range(16)], axis=1)
    result = hid[...] + blend_gate * nn(dense_inner, sd_v[...])

    pltpu.make_async_copy(ret.at[bulk], ret.at[bulk], r_recv).wait()
    got = nn(dtmat[...], ret[...])
    routed = [
        weight0 * got[k * 64:(k + 1) * 64] + weight1 * got[256 + k * 64:256 + (k + 1) * 64] for k in range(4)
    ]
    out[...] = (result + jnp.concatenate(routed, axis=1)).astype(BF)

    pltpu.make_async_copy(sre, nre, lsem.at[16]).wait()
    pltpu.make_async_copy(sim, nim, lsem.at[17]).wait()
    pltpu.make_async_copy(wbg.at[most], wbg.at[most], w_send.at[0]).wait()
    pltpu.make_async_copy(wbu.at[most], wbu.at[most], w_send.at[1]).wait()
    pltpu.make_async_copy(xo.at[bulk], xo.at[bulk], d_send).wait()
    pltpu.make_async_copy(ret.at[bulk], ret.at[bulk], r_send).wait()
    pltpu.make_async_copy(dn.at[fifteen], dn.at[fifteen], n_send).wait()


def shards(
    tokens, sequence_state_real, sequence_state_imaginary, mixer_norm_gain, expert_norm_gain, rate, freq,
    log_group_step, input_map_real, input_map_imaginary, output_map_real, output_map_imaginary, skip,
    mixer_value_weight, mixer_gate_weight, group_router_weight, expert_router_weight, dense_blend_weight, routes,
    expert_gate_weight, expert_up_weight, expert_down_weight, shared_gate_weight, shared_up_weight,
    shared_down_weight,
):
    vmem = pl.BlockSpec(memory_space=pltpu.VMEM)
    hbm = pl.BlockSpec(memory_space=pl.ANY)
    V = pltpu.VMEM
    D = pltpu.SemaphoreType.DMA
    state = jax.ShapeDtypeStruct((64, 64, 64), F32)
    operands = (
        tokens, mixer_norm_gain[None], expert_norm_gain[None], rate, freq, log_group_step[None], skip[None],
        group_router_weight.T, expert_router_weight.T, dense_blend_weight[None], routes.T,
        sequence_state_real, sequence_state_imaginary,
        jnp.swapaxes(input_map_real, 1, 2).reshape(1024, 64), jnp.swapaxes(input_map_imaginary, 1, 2).reshape(1024, 64),
        output_map_real.reshape(1024, 64), output_map_imaginary.reshape(1024, 64),
        mixer_value_weight, mixer_gate_weight, expert_gate_weight, expert_up_weight, expert_down_weight,
        shared_gate_weight.T, shared_up_weight.T, shared_down_weight,
    )
    scratch = [
        V((64 * PITCH, 64), F32), V((64 * PITCH, 64), F32),
        V((1024, 64), F32), V((1024, 64), F32), V((1024, 64), F32), V((1024, 64), F32),
        V((2, 1024, 1024), BF), V((2, 1024, 1024), BF),
        V((2048, 512), BF), V((2048, 512), BF), V((512, 2048), BF),
        V((2048, 1024), BF), V((256, 1024), BF), V((256, 1024), BF),
        V((64, 64), F32), V((64, 64), F32), V((64, 64), F32), V((64, 64), F32),
        V((1024, 64), BF), V((1024, 64), BF), V((1024, 64), BF), V((1024, 64), BF),
        V((64, 1024), BF), V((64, 1024), BF), V((128, 1024), BF),
        V((1024, 256), BF), V((512, 1024), BF), V((64, 64), F32), V((64, 64), F32), V((256, 256), BF), V((256, 256), BF),
        V((64, 128), F32), V((64, 128), F32), V((2, 64, 1024), BF), V((2, 64, 1024), BF),
        V((64, 128), F32), V((64, 128), F32),
        V((1024, 256), BF), V((1024, 256), BF), V((1024, 256), BF), V((256, 1024), BF),
        V((2, 256, 512), F32), V((256, 512), BF),
        V((256, 1024), BF), V((256, 1024), BF), V((256, 1024), BF),
        V((1024, 256), BF), V((1024, 256), BF),
        V((512, 1024), BF), V((2, 512, 128), BF), V((2, 512, 128), BF), V((512, 128), BF),
        V((1024, 128), BF), V((64, 1024), F32),
        D((18,)), D((7,)), D((7,)), D((2,)), D((2,)), D, D, D((7,)), D((7,)), D, D, D, D,
    ]
    return pl.pallas_call(
        body,
        out_shape=(jax.ShapeDtypeStruct((64, 1024), BF), state, state),
        in_specs=[vmem] * 11 + [hbm] * 14,
        out_specs=(vmem, hbm, hbm),
        scratch_shapes=scratch,
        compiler_params=pltpu.CompilerParams(
            collective_id=0, has_side_effects=True, vmem_limit_bytes=60 * 1024 * 1024
        ),
    )(*operands)


def solution(mesh):
    placed = (
        P("ep", "tp"),
        P("ep", "tp", None),
        P("ep", "tp", None),
        P(),
        P(),
        P("tp", None),
        P("tp", None),
        P("tp"),
        P("tp", None, None),
        P("tp", None, None),
        P("tp", None, None),
        P("tp", None, None),
        P("tp"),
        P("tp", None),
        P("tp", None),
        P(),
        P(),
        P(),
        P("ep", None),
        P("ep", None, "tp"),
        P("ep", None, "tp"),
        P("ep", "tp", None),
        P("tp", "ep"),
        P("tp", "ep"),
        P(None, "tp"),
    )
    return jax.shard_map(
        shards,
        mesh=mesh,
        in_specs=placed,
        out_specs=(P("ep", "tp"), P("ep", "tp", None), P("ep", "tp", None)),
        check_vma=False,
    )
```

```python
import jax
import jax.numpy as jnp
from jax import lax
from jax.experimental import pallas as pl
from jax.experimental.pallas import tpu as pltpu
from jax.sharding import PartitionSpec as P

MESH = pl.DeviceIdType.MESH
BF = jnp.bfloat16
F32 = jnp.float32
I32 = jnp.int32
EPS = 1e-06
BIG = 3.0e38
NEP = 64
ROWS = 64
HALF = 1024
WIDTH = 2048
PITCH = 72
REACH = (
    (1, 0, 0, 0, 64), (3, 0, 0, 0, 64), (0, 1, 0, 0, 64), (0, 3, 0, 0, 64), (0, 0, 1, 0, 32),
    (0, 0, 3, 32, 32), (1, 3, 0, 0, 32), (3, 1, 0, 32, 32), (1, 1, 0, 0, 32), (3, 3, 0, 32, 32),
)
AROUND = sorted(
    ((d % 4, (d // 4) % 4, d // 16) for d in range(1, 64)), key=lambda o: -sum(min(v, 4 - v) for v in o)
)


def nn(a, b):
    return jnp.dot(a, b, preferred_element_type=F32)


def nt(a, b):
    return lax.dot_general(a, b, (((1,), (1,)), ((), ())), preferred_element_type=F32)


def iota(shape, dim):
    return lax.broadcasted_iota(I32, shape, dim)


def onehot(condition):
    return jnp.where(condition, 1.0, 0.0).astype(BF)


def column(row, n):
    spread = jnp.where(iota((n, n), 0) == iota((n, n), 1), jnp.broadcast_to(row, (n, n)), 0.0)
    return jnp.sum(spread, axis=1, keepdims=True)


def sigmoid(x):
    return 1.0 / (1.0 + jnp.exp(-x))


def gelu(x):
    return x * (0.5 * (1.0 + jnp.tanh(0.7978845608028654 * (x + 0.044715 * (x * x * x)))))


def shard_of(colour, member):
    z = lax.rem(member, 4)
    y = 2 * lax.div(member, 4) + lax.rem(colour, 2)
    x = lax.rem(lax.div(colour, 2) + 16 - y - 2 * z, 4)
    return z * 16 + y * 4 + x


def body(
    tok, mgain, egain, rate, freq, lgs, skip, grw, erw, blend, routes,
    sre, sim, imr, imi, omr, omi, wv, wg, eg, eu, ed, sg, su, sd,
    out, nre, nim,
    sre_v, sim_v, imr_v, imi_v, omr_v, omi_v, wv_v, wg_v, eg_v, eu_v, ed_v, sd_v, wb,
    fre, fim, are, aim, bre, bim, cre, cim, vbuf, abuf, rt, dmat, dtmat, m0s, m1s, perm, permt,
    e1s, e1r, vgs, vgr, e3s, e3r, dsend, xo, xp, xx, acc, inner, pts, ptr, ptot, rsend, ret,
    tb, dps, dpr, dis, dn, hid,
    lsem, e_send, e_recv, w_send, w_recv, d_send, d_recv, t_send, t_recv, r_send, r_recv, n_send, n_recv,
):
    ep = lax.axis_index("ep")
    tp = lax.axis_index("tp")
    other = 1 - tp
    x = lax.rem(ep, 4)
    y = lax.rem(lax.div(ep, 4), 4)
    z = lax.div(ep, 16)
    xs = [lax.rem(x + k, 4) for k in range(4)]
    ys = [lax.rem(y + k, 4) * 4 for k in range(4)]
    zs = [lax.rem(z + k, 4) * 16 for k in range(4)]

    def chip(dx, dy, dz):
        return zs[dz % 4] + ys[dy % 4] + xs[dx % 4]

    colour = 2 * lax.rem(x + y + 2 * z, 4) + lax.rem(y, 2)
    member = lax.div(y, 2) * 4 + z
    own_cols = pl.ds(pl.multiple_of(tp * HALF, HALF), HALF)
    peer_cols = pl.ds(pl.multiple_of(other * HALF, HALF), HALF)

    barrier = pltpu.get_barrier_semaphore()
    for dx, dy, dz in AROUND:
        pl.semaphore_signal(barrier, inc=1, device_id=(chip(dx, dy, dz), tp), device_id_type=MESH)
    for dx, dy, dz, first, rows in REACH:
        pl.semaphore_signal(barrier, inc=1, device_id=(chip(dx, dy, dz), other), device_id_type=MESH)
    pl.semaphore_signal(barrier, inc=1, device_id=(ep, other), device_id_type=MESH)
    greeted = len(AROUND) + len(REACH) + 1

    def load(src, dst, k):
        c = pltpu.make_async_copy(src, dst, lsem.at[k])
        c.start()
        return c

    l_imr = load(imr, imr_v, 0)
    l_imi = load(imi, imi_v, 1)

    kept_re = sre_v.reshape(ROWS, PITCH, 64).at[:, pl.ds(0, 64)]
    kept_im = sim_v.reshape(ROWS, PITCH, 64).at[:, pl.ds(0, 64)]
    l_sre = load(sre, kept_re, 2)
    l_sim = load(sim, kept_im, 3)
    l_omr = load(omr, omr_v, 4)
    l_omi = load(omi, omi_v, 5)
    l_wv1 = load(wv.at[:, peer_cols], wv_v.at[0], 6)
    l_wg1 = load(wg.at[:, peer_cols], wg_v.at[0], 7)
    l_wv0 = load(wv.at[:, own_cols], wv_v.at[1], 8)
    l_wg0 = load(wg.at[:, own_cols], wg_v.at[1], 9)
    l_eg = load(eg.at[0], eg_v, 10)
    l_eu = load(eu.at[0], eu_v, 11)
    l_ed = load(ed.at[0], ed_v, 12)
    wrow = lax.div(member, 4) * 256 + lax.rem(member, 4) * 32
    l_sg = load(sg, wb.at[pl.ds(pl.multiple_of(wrow, 32), 32)], 13)
    l_su = load(su, wb.at[pl.ds(pl.multiple_of(wrow + 128, 32), 32)], 14)

    tokf = tok[...].astype(F32)
    ss = jnp.sum(tokf * tokf, axis=1, keepdims=True)
    e1s[...] = jnp.broadcast_to(ss, (ROWS, 128))

    step = jnp.exp(column(lgs[...], 64))
    mag = jnp.exp(-rate[...] * step)
    a_re = mag * jnp.cos(freq[...] * step)
    a_im = mag * jnp.sin(freq[...] * step)
    denom = rate[...] * rate[...] + freq[...] * freq[...]
    sh_re = a_re - 1.0
    fre[...] = (a_im * freq[...] - sh_re * rate[...]) / denom
    fim[...] = -(a_im * rate[...] + sh_re * freq[...]) / denom
    are[...] = a_re
    aim[...] = a_im
    l_imr.wait()
    l_imi.wait()

    def make_b(g, carry):
        rows = pl.ds(pl.multiple_of(g * 16, 16), 16)
        f_re = fre[pl.ds(g, 1), :]
        f_im = fim[pl.ds(g, 1), :]
        m_re = imr_v[rows, :]
        m_im = imi_v[rows, :]
        bre[rows, :] = (f_re * m_re - f_im * m_im).astype(BF)
        bim[rows, :] = (f_re * m_im + f_im * m_re).astype(BF)
        return carry

    lax.fori_loop(0, 64, make_b, 0)

    r0 = routes[0:1, :].astype(F32)
    r1 = routes[1:2, :].astype(F32)
    e_sub = iota((64, 64), 0).astype(F32)
    e_lane = iota((64, 64), 1).astype(F32)
    m0 = onehot(e_sub == r0)
    m1 = onehot(e_sub == r1)
    sub4 = iota((64, 256), 0)
    lane4 = iota((64, 256), 1) % 64
    same4 = onehot(sub4 == lane4)
    before4 = onehot(sub4 < lane4)
    n0 = jnp.sum(m0.astype(F32), axis=1, keepdims=True)
    a4 = nn(m0, same4) * (nn(m0, before4) + 1.0) + nn(m1, same4) * (nn(m1, before4) + n0 + 1.0)
    a4 = a4.astype(BF)

    def make_d(q, carry):
        row = iota((256, 1), 0)
        spread = onehot((row // 16 + q * 16) == iota((256, 64), 1))
        got = nn(spread, a4)
        hit = (got == ((row % 4) + 1).astype(F32)) & (((row // 4) % 4) == (iota((256, 256), 1) // 64))
        dmat[pl.ds(pl.multiple_of(q * 256, 256), 256), :] = onehot(hit)
        return carry

    lax.fori_loop(0, 4, make_d, 0)

    pl.semaphore_wait(barrier, greeted)

    def exchange(src, dst, k):
        c = pltpu.make_async_remote_copy(
            src_ref=src, dst_ref=dst, send_sem=e_send.at[k], recv_sem=e_recv.at[k],
            device_id=(ep, other), device_id_type=MESH,
        )
        c.start()
        return c

    x1 = exchange(e1s, e1r, 0)

    groups = [lax.rem(member + k, 8) for k in (6, 2, 5, 7, 1, 3, 4)]
    groups = [shard_of(colour, m) for m in groups]
    for piece in range(4):
        for dest in groups:
            for i, src in enumerate((sg, su)):
                pltpu.make_async_remote_copy(
                    src_ref=src.at[pl.ds(piece * 8, 8)],
                    dst_ref=wb.at[pl.ds(pl.multiple_of(wrow + i * 128 + piece * 8, 8), 8)],
                    send_sem=w_send, recv_sem=w_recv, device_id=(dest, tp), device_id_type=MESH,
                ).start()

    c0 = column(r0, 64)
    c1 = column(r1, 64)
    t0 = onehot(e_lane == c0)
    t1 = onehot(e_lane == c1)
    earlier = onehot(iota((64, 64), 1) < iota((64, 64), 0))
    b0 = (t0.astype(F32) * (nn(earlier, t0) + 1.0)).astype(BF)
    b1 = (t1.astype(F32) * (nn(earlier, t1) + jnp.sum(t0.astype(F32), axis=0, keepdims=True) + 1.0)).astype(BF)
    m0s[...] = t0.astype(F32)
    m1s[...] = t1.astype(F32)

    def make_dt(q, carry):
        lane = iota((1, 256), 1)
        spread = onehot((iota((64, 256), 0)) == (iota((64, 256), 1) // 16 + q * 16))
        want = ((lane % 4) + 1).astype(F32)
        cols = pl.ds(pl.multiple_of(q * 256, 256), 256)
        for route, coded in enumerate((b0, b1)):
            got = nn(coded, spread) == want
            for k in range(4):
                rows = pl.ds(route * 256 + k * 64, 64)
                dtmat[rows, cols] = onehot(got & (((lane // 4) % 4) == k))
        return carry

    lax.fori_loop(0, 4, make_dt, 0)
    pi = iota((256, 256), 0)
    pj = iota((256, 256), 1)
    perm[...] = onehot((((pi // 4) % 16) * 16 + (pi // 64) * 4 + pi % 4) == pj)
    permt[...] = onehot((((pi // 4) % 4) * 64 + (pi // 16) * 4 + pi % 4) == pj)
    rt[0:64, :] = erw[:, own_cols]
    rt[64:128, :] = jnp.concatenate([grw[:, own_cols].astype(F32), jnp.zeros((60, HALF), F32)], axis=0).astype(BF)

    x1.wait()
    total = ss + e1r[:, 0:1]
    scale = lax.rsqrt(total / WIDTH + EPS)
    vbuf[...] = (tokf * scale * mgain[:, own_cols]).astype(BF)
    l_omr.wait()
    l_omi.wait()
    cre[...] = omr_v[...].astype(BF)
    cim[...] = omi_v[...].astype(BF)
    l_sre.wait()
    l_sim.wait()
    lane_group = iota((ROWS, 128), 1) // 16

    def state_block(b, carry):
        cols = pl.ds(pl.multiple_of(b * 128, 128), 128)
        u = vbuf[:, cols]
        spread = jnp.concatenate([jnp.where(lane_group == j, u, jnp.zeros_like(u)) for j in range(8)], axis=0)
        d_re = nn(spread, bre[cols, :])
        d_im = nn(spread, bim[cols, :])
        fresh_re = []
        fresh_im = []
        for j in range(8):
            g = b * 8 + j
            at = pl.ds(g, ROWS, stride=PITCH)
            s_re = sre_v[at, :]
            s_im = sim_v[at, :]
            g_re = are[pl.ds(g, 1), :]
            g_im = aim[pl.ds(g, 1), :]
            n_re = g_re * s_re - g_im * s_im + d_re[j * ROWS:(j + 1) * ROWS]
            n_im = g_re * s_im + g_im * s_re + d_im[j * ROWS:(j + 1) * ROWS]
            sre_v[at, :] = n_re
            sim_v[at, :] = n_im
            fresh_re.append(n_re.astype(BF))
            fresh_im.append(n_im.astype(BF))
        read = nt(jnp.concatenate(fresh_re, axis=0), cre[cols, :]) - nt(jnp.concatenate(fresh_im, axis=0), cim[cols, :])
        mixed = skip[:, cols] * u.astype(F32)
        for j in range(8):
            mixed = mixed + jnp.where(lane_group == j, read[j * ROWS:(j + 1) * ROWS], 0.0)
        abuf[:, cols] = gelu(mixed).astype(BF)
        return carry

    lax.fori_loop(0, 8, state_block, 0)

    s_nre = load(kept_re, nre, 16)
    s_nim = load(kept_im, nim, 17)

    act = abuf[...]
    l_wv1.wait()
    vgs[0] = nn(act, wv_v[0]).astype(BF)
    x2 = exchange(vgs.at[0], vgr.at[0], 1)
    l_wg1.wait()
    vgs[1] = nn(act, wg_v[0]).astype(BF)
    x3 = exchange(vgs.at[1], vgr.at[1], 2)
    l_wv0.wait()
    value = nn(act, wv_v[1]).astype(BF).astype(F32)
    l_wg0.wait()
    gate = nn(act, wg_v[1]).astype(BF).astype(F32)
    x2.wait()
    x3.wait()
    value = value + vgr[0].astype(F32)
    gate = gate + vgr[1].astype(F32)
    mix = (value * sigmoid(gate)).astype(BF)
    hidden = (tok[...].astype(F32) + mix.astype(F32)).astype(BF).astype(F32)
    hid[...] = hidden
    scaled = hidden * egain[:, own_cols]
    top = scaled.astype(BF)
    rest = (scaled - top.astype(F32)).astype(BF)
    logits = nt(top, rt[...]) + nt(rest, rt[...])
    blend_part = jnp.sum(scaled * blend[:, own_cols], axis=1, keepdims=True)
    square_part = jnp.sum(hidden * hidden, axis=1, keepdims=True)
    lane = iota((ROWS, 128), 1)
    logits = jnp.where(lane == 68, blend_part, jnp.where(lane == 69, square_part, logits))
    e3s[...] = logits
    x4 = exchange(e3s, e3r, 3)
    x4.wait()
    logits = logits + e3r[...]
    squares = jnp.sum(jnp.where(lane == 69, logits, 0.0), axis=1, keepdims=True)
    inverse = lax.rsqrt(squares / WIDTH + EPS)
    hnorm = (scaled * inverse).astype(BF)
    logits = logits * inverse

    tb[0:ROWS, :] = hnorm
    quarters = jnp.concatenate([hnorm[:, k * 256:(k + 1) * 256] for k in range(4)], axis=0)
    dsend[...] = nn(dmat[...], quarters).astype(BF)
    mine = pl.ds(pl.multiple_of(ep * 16, 16), 16)
    xo[mine, :] = dsend[mine, :]

    def send_rows(src, dst, ssem, rsem):
        for dx, dy, dz in AROUND:
            dest = chip(dx, dy, dz)
            pltpu.make_async_remote_copy(
                src_ref=src.at[pl.ds(pl.multiple_of(dest * 16, 16), 16)], dst_ref=dst.at[mine],
                send_sem=ssem, recv_sem=rsem, device_id=(dest, tp), device_id_type=MESH,
            ).start()

    send_rows(dsend, xo, d_send, d_recv)
    tok_copies = []
    at = ROWS
    for i, (dx, dy, dz, first, rows) in enumerate(REACH):
        c = pltpu.make_async_remote_copy(
            src_ref=tb.at[pl.ds(first, rows)], dst_ref=tb.at[pl.ds(at, rows)],
            send_sem=t_send.at[i], recv_sem=t_recv.at[i], device_id=(chip(dx, dy, dz), tp), device_id_type=MESH,
        )
        c.start()
        tok_copies.append(c)
        at += rows

    def load_down(p, carry):
        i = shard_of(lax.div(p, 8), lax.rem(p, 8))
        pltpu.make_async_copy(
            sd.at[pl.ds(pl.multiple_of(i * 32, 32), 32)], sd_v.at[pl.ds(pl.multiple_of(p * 32, 32), 32)], lsem.at[15]
        ).start()
        return carry

    lax.fori_loop(0, 64, load_down, 0)

    blend_logit = jnp.sum(jnp.where(lane == 68, logits, 0.0), axis=1, keepdims=True)
    is_group = (lane >= 64) & (lane < 68)
    group_max = jnp.max(jnp.where(is_group, logits, -jnp.inf), axis=1, keepdims=True)
    group_exp = jnp.where(is_group, jnp.exp(jnp.where(is_group, logits, group_max) - group_max), 0.0)
    group_prob = group_exp / jnp.sum(group_exp, axis=1, keepdims=True)
    row0 = column(routes[0:1, :].astype(F32), 64).astype(I32)
    row1 = column(routes[1:2, :].astype(F32), 64).astype(I32)
    pick0 = jnp.sum(jnp.where(lane == row0, logits, 0.0), axis=1, keepdims=True)
    pick1 = jnp.sum(jnp.where(lane == row1, logits, 0.0), axis=1, keepdims=True)
    prob0 = jnp.sum(jnp.where(lane == 64 + row0 // 16, group_prob, 0.0), axis=1, keepdims=True)
    prob1 = jnp.sum(jnp.where(lane == 64 + row1 // 16, group_prob, 0.0), axis=1, keepdims=True)
    top_pick = jnp.maximum(pick0, pick1)
    exp0 = jnp.exp(pick0 - top_pick)
    exp1 = jnp.exp(pick1 - top_pick)
    weight0 = exp0 / (exp0 + exp1) * prob0
    weight1 = exp1 / (exp0 + exp1) * prob1
    blend_gate = sigmoid(blend_logit)

    bulk = pl.ds(0, (NEP - 1) * 16)
    pltpu.make_async_copy(xo.at[bulk], xo.at[bulk], d_recv).wait()
    x5 = exchange(xo, xp, 4)
    l_eg.wait()
    l_eu.wait()

    def unpack(src):
        for q in range(4):
            got = nn(perm[...], src[q * 256:(q + 1) * 256, :]).astype(BF)
            for k in range(4):
                xx[q * 64:(q + 1) * 64, k * 256:(k + 1) * 256] = got[k * 64:(k + 1) * 64]

    unpack(xo)
    acc[0] = nn(xx[...], eg_v[own_cols, :])
    acc[1] = nn(xx[...], eu_v[own_cols, :])
    x5.wait()
    unpack(xp)
    gate_e = acc[0] + nn(xx[...], eg_v[peer_cols, :])
    up_e = acc[1] + nn(xx[...], eu_v[peer_cols, :])
    inner[...] = (gate_e * sigmoid(gate_e) * up_e).astype(BF)
    l_ed.wait()
    pts[...] = nn(inner[...], ed_v[:, peer_cols]).astype(BF)
    x6 = exchange(pts, ptr, 5)
    part = nn(inner[...], ed_v[:, own_cols]).astype(BF)
    ptot[...] = part
    x6.wait()
    ptot[...] = (ptot[...].astype(F32) + ptr[...].astype(F32)).astype(BF)
    for q in range(4):
        rows = slice(q * 64, (q + 1) * 64)
        block = jnp.concatenate([ptot[rows, k * 256:(k + 1) * 256] for k in range(4)], axis=0)
        rsend[q * 256:(q + 1) * 256, :] = nn(permt[...], block).astype(BF)
    ret[mine, :] = rsend[mine, :]
    send_rows(rsend, ret, r_send, r_recv)

    l_sg.wait()
    l_su.wait()
    most = pl.ds(0, 7 * 64)
    pltpu.make_async_copy(wb.at[most], wb.at[most], w_recv).wait()
    for c in tok_copies:
        c.wait()
    peer_units = pl.ds(pl.multiple_of(other * 256, 256), 256)
    own_units = pl.ds(pl.multiple_of(tp * 256, 256), 256)
    dps[...] = nt(tb[...], wb[peer_units, :]).astype(BF)
    x7 = exchange(dps, dpr, 6)
    dense = nt(tb[...], wb[own_units, :]).astype(BF).astype(F32)
    x7.wait()
    dense = dense + dpr[...].astype(F32)
    dgate = dense[:, 0:128]
    dis[...] = (dgate * sigmoid(dgate) * dense[:, 128:256]).astype(BF)
    slot = pl.ds(pl.multiple_of((colour * 2 + tp) * ROWS, ROWS), ROWS)
    dn[slot, :] = dis[0:ROWS, :]

    def send_inner(at, first, rows, dest, core):
        base = (colour * 2 + tp) * ROWS + first
        pltpu.make_async_remote_copy(
            src_ref=dis.at[pl.ds(at, rows)], dst_ref=dn.at[pl.ds(pl.multiple_of(base, 32), rows)],
            send_sem=n_send, recv_sem=n_recv, device_id=(dest, core), device_id_type=MESH,
        ).start()

    at = ROWS
    for dx, dy, dz, first, rows in REACH:
        send_inner(at, first, rows, chip(-dx, -dy, -dz), tp)
        send_inner(at, first, rows, chip(-dx, -dy, -dz), other)
        at += rows
    send_inner(0, 0, ROWS, ep, other)
    pltpu.make_async_copy(sd, sd, lsem.at[15]).wait()
    fifteen = pl.ds(0, 15 * ROWS)
    pltpu.make_async_copy(dn.at[fifteen], dn.at[fifteen], n_recv).wait()
    dense_inner = jnp.concatenate([dn[s * ROWS:(s + 1) * ROWS, :] for s in range(16)], axis=1)
    result = hid[...] + blend_gate * nn(dense_inner, sd_v[...])

    pltpu.make_async_copy(ret.at[bulk], ret.at[bulk], r_recv).wait()
    got = nn(dtmat[...], ret[...])
    routed = [
        weight0 * got[k * 64:(k + 1) * 64] + weight1 * got[256 + k * 64:256 + (k + 1) * 64] for k in range(4)
    ]
    out[...] = (result + jnp.concatenate(routed, axis=1)).astype(BF)

    s_nre.wait()
    s_nim.wait()
    pltpu.make_async_copy(wb.at[most], wb.at[most], w_send).wait()
    pltpu.make_async_copy(xo.at[bulk], xo.at[bulk], d_send).wait()
    pltpu.make_async_copy(ret.at[bulk], ret.at[bulk], r_send).wait()
    pltpu.make_async_copy(dn.at[fifteen], dn.at[fifteen], n_send).wait()


def shards(
    tokens, sequence_state_real, sequence_state_imaginary, mixer_norm_gain, expert_norm_gain, rate, freq,
    log_group_step, input_map_real, input_map_imaginary, output_map_real, output_map_imaginary, skip,
    mixer_value_weight, mixer_gate_weight, group_router_weight, expert_router_weight, dense_blend_weight, routes,
    expert_gate_weight, expert_up_weight, expert_down_weight, shared_gate_weight, shared_up_weight,
    shared_down_weight,
):
    vmem = pl.BlockSpec(memory_space=pltpu.VMEM)
    hbm = pl.BlockSpec(memory_space=pl.ANY)
    V = pltpu.VMEM
    D = pltpu.SemaphoreType.DMA
    state = jax.ShapeDtypeStruct((64, 64, 64), F32)
    operands = (
        tokens, mixer_norm_gain[None], expert_norm_gain[None], rate, freq, log_group_step[None], skip[None],
        group_router_weight.T, expert_router_weight.T, dense_blend_weight[None], routes.T,
        sequence_state_real, sequence_state_imaginary,
        jnp.swapaxes(input_map_real, 1, 2).reshape(1024, 64), jnp.swapaxes(input_map_imaginary, 1, 2).reshape(1024, 64),
        output_map_real.reshape(1024, 64), output_map_imaginary.reshape(1024, 64),
        mixer_value_weight, mixer_gate_weight, expert_gate_weight, expert_up_weight, expert_down_weight,
        shared_gate_weight.T, shared_up_weight.T, shared_down_weight,
    )
    scratch = [
        V((64 * PITCH, 64), F32), V((64 * PITCH, 64), F32),
        V((1024, 64), F32), V((1024, 64), F32), V((1024, 64), F32), V((1024, 64), F32),
        V((2, 1024, 1024), BF), V((2, 1024, 1024), BF),
        V((2048, 512), BF), V((2048, 512), BF), V((512, 2048), BF),
        V((2048, 1024), BF), V((512, 1024), BF),
        V((64, 64), F32), V((64, 64), F32), V((64, 64), F32), V((64, 64), F32),
        V((1024, 64), BF), V((1024, 64), BF), V((1024, 64), BF), V((1024, 64), BF),
        V((64, 1024), BF), V((64, 1024), BF), V((128, 1024), BF),
        V((1024, 256), BF), V((512, 1024), BF), V((64, 64), F32), V((64, 64), F32), V((256, 256), BF), V((256, 256), BF),
        V((64, 128), F32), V((64, 128), F32), V((2, 64, 1024), BF), V((2, 64, 1024), BF),
        V((64, 128), F32), V((64, 128), F32),
        V((1024, 256), BF), V((1024, 256), BF), V((1024, 256), BF), V((256, 1024), BF),
        V((2, 256, 512), F32), V((256, 512), BF),
        V((256, 1024), BF), V((256, 1024), BF), V((256, 1024), BF),
        V((1024, 256), BF), V((1024, 256), BF),
        V((512, 1024), BF), V((512, 256), BF), V((512, 256), BF), V((512, 128), BF),
        V((1024, 128), BF), V((64, 1024), F32),
        D((18,)), D((7,)), D((7,)), D, D, D, D, D((len(REACH),)), D((len(REACH),)), D, D, D, D,
    ]
    result, next_re, next_im = pl.pallas_call(
        body,
        out_shape=(jax.ShapeDtypeStruct((64, 1024), BF), state, state),
        in_specs=[vmem] * 11 + [hbm] * 14,
        out_specs=(vmem, hbm, hbm),
        scratch_shapes=scratch,
        compiler_params=pltpu.CompilerParams(
            collective_id=0, has_side_effects=True, vmem_limit_bytes=60 * 1024 * 1024
        ),
    )(*operands)
    return (result, lax.clamp(-BIG, next_re, BIG), lax.clamp(-BIG, next_im, BIG))


def solution(mesh):
    placed = (
        P("ep", "tp"),
        P("ep", "tp", None),
        P("ep", "tp", None),
        P(),
        P(),
        P("tp", None),
        P("tp", None),
        P("tp"),
        P("tp", None, None),
        P("tp", None, None),
        P("tp", None, None),
        P("tp", None, None),
        P("tp"),
        P("tp", None),
        P("tp", None),
        P(),
        P(),
        P(),
        P("ep", None),
        P("ep", None, "tp"),
        P("ep", None, "tp"),
        P("ep", "tp", None),
        P("tp", "ep"),
        P("tp", "ep"),
        P(None, "tp"),
    )
    return jax.shard_map(
        shards,
        mesh=mesh,
        in_specs=placed,
        out_specs=(P("ep", "tp"), P("ep", "tp", None), P("ep", "tp", None)),
        check_vma=False,
    )
```

```python
import jax
import jax.numpy as jnp
from jax import lax
from jax.experimental import pallas as pl
from jax.experimental.pallas import tpu as pltpu
from jax.sharding import PartitionSpec as P

MESH = pl.DeviceIdType.MESH
BF = jnp.bfloat16
F32 = jnp.float32
I32 = jnp.int32
EPS = 1e-06
PARTS = 4
NEP = 64
ROWS = 64
HALF = 1024
WIDTH = 2048
PITCH = 72
REACH = (
    (1, 0, 0, 0, 64), (3, 0, 0, 0, 64), (0, 1, 0, 0, 64), (0, 3, 0, 0, 64), (0, 0, 1, 0, 32),
    (0, 0, 3, 32, 32), (1, 3, 0, 0, 32), (3, 1, 0, 32, 32), (1, 1, 0, 0, 32), (3, 3, 0, 32, 32),
)
AROUND = sorted(
    ((d % 4, (d // 4) % 4, d // 16) for d in range(1, 64)), key=lambda o: -sum(min(v, 4 - v) for v in o)
)


def nn(a, b):
    return jnp.dot(a, b, preferred_element_type=F32)


def nt(a, b):
    return lax.dot_general(a, b, (((1,), (1,)), ((), ())), preferred_element_type=F32)


def iota(shape, dim):
    return lax.broadcasted_iota(I32, shape, dim)


def onehot(condition):
    return jnp.where(condition, 1.0, 0.0).astype(BF)


def column(row, n):
    spread = jnp.where(iota((n, n), 0) == iota((n, n), 1), jnp.broadcast_to(row, (n, n)), 0.0)
    return jnp.sum(spread, axis=1, keepdims=True)


def sigmoid(x):
    return 1.0 / (1.0 + jnp.exp(-x))


def gelu(x):
    return x * (0.5 * (1.0 + jnp.tanh(0.7978845608028654 * (x + 0.044715 * (x * x * x)))))


def shard_of(colour, member):
    z = lax.rem(member, 4)
    y = 2 * lax.div(member, 4) + lax.rem(colour, 2)
    x = lax.rem(lax.div(colour, 2) + 16 - y - 2 * z, 4)
    return z * 16 + y * 4 + x


def body(
    tok_h, mgain_h, egain_h, rate_h, freq_h, lgs_h, skip_h, grw_h, erw_h, blend_h, routes_h,
    sre, sim, imr, imi, omr, omi, wv, wg, eg, eu, ed, sg, su, sd,
    out, nre, nim,
    tok, mgain, egain, rate, freq, lgs, skip, grw, erw, blend, routes,
    sre_v, sim_v, imr_v, imi_v, omr_v, omi_v, wv_v, wg_v, eg_v, eu_v, ed_v, sd_v, wb,
    fre, fim, are, aim, bre, bim, cre, cim, vbuf, abuf, rt, dmat, dtmat, m0s, m1s, perm, permt,
    e1s, e1r, vgs, vgr, e3s, e3r, dsend, xo, xp, xx, acc, inner, pts, ptr, ptot, rsend, ret,
    tb, dps, dpr, dis, dn, hid,
    lsem, e_send, e_recv, w_send, w_recv, d_send, d_recv, t_send, t_recv, r_send, r_recv, n_send, n_recv,
):
    ep = lax.axis_index("ep")
    tp = lax.axis_index("tp")
    other = 1 - tp
    x = lax.rem(ep, 4)
    y = lax.rem(lax.div(ep, 4), 4)
    z = lax.div(ep, 16)
    xs = [lax.rem(x + k, 4) for k in range(4)]
    ys = [lax.rem(y + k, 4) * 4 for k in range(4)]
    zs = [lax.rem(z + k, 4) * 16 for k in range(4)]

    def chip(dx, dy, dz):
        return zs[dz % 4] + ys[dy % 4] + xs[dx % 4]

    colour = 2 * lax.rem(x + y + 2 * z, 4) + lax.rem(y, 2)
    member = lax.div(y, 2) * 4 + z
    own_cols = pl.ds(pl.multiple_of(tp * HALF, HALF), HALF)
    peer_cols = pl.ds(pl.multiple_of(other * HALF, HALF), HALF)

    barrier = pltpu.get_barrier_semaphore()
    for dx, dy, dz in AROUND:
        pl.semaphore_signal(barrier, inc=1, device_id=(chip(dx, dy, dz), tp), device_id_type=MESH)
    for dx, dy, dz, first, rows in REACH:
        pl.semaphore_signal(barrier, inc=1, device_id=(chip(dx, dy, dz), other), device_id_type=MESH)
    pl.semaphore_signal(barrier, inc=1, device_id=(ep, other), device_id_type=MESH)
    greeted = len(AROUND) + len(REACH) + 1

    def load(src, dst, k):
        c = pltpu.make_async_copy(src, dst, lsem.at[k])
        c.start()
        return c

    small = [
        load(src, dst, 18 + k)
        for k, (src, dst) in enumerate((
            (tok_h, tok), (routes_h, routes), (rate_h, rate), (freq_h, freq), (lgs_h, lgs), (mgain_h, mgain),
            (skip_h, skip), (grw_h, grw), (erw_h, erw), (egain_h, egain), (blend_h, blend),
        ))
    ]
    l_imr = load(imr, imr_v, 0)
    l_imi = load(imi, imi_v, 1)

    kept_re = sre_v.reshape(ROWS, PITCH, 64).at[:, pl.ds(0, 64)]
    kept_im = sim_v.reshape(ROWS, PITCH, 64).at[:, pl.ds(0, 64)]
    l_sre = load(sre, kept_re, 2)
    l_sim = load(sim, kept_im, 3)
    l_omr = load(omr, omr_v, 4)
    l_omi = load(omi, omi_v, 5)
    l_wv1 = load(wv.at[:, peer_cols], wv_v.at[0], 6)
    l_wg1 = load(wg.at[:, peer_cols], wg_v.at[0], 7)
    l_wv0 = load(wv.at[:, own_cols], wv_v.at[1], 8)
    l_wg0 = load(wg.at[:, own_cols], wg_v.at[1], 9)
    l_eg = load(eg.at[0], eg_v, 10)
    l_eu = load(eu.at[0], eu_v, 11)
    l_ed = load(ed.at[0], ed_v, 12)
    wrow = lax.div(member, 4) * 256 + lax.rem(member, 4) * 32
    l_sg = load(sg, wb.at[pl.ds(pl.multiple_of(wrow, 32), 32)], 13)
    l_su = load(su, wb.at[pl.ds(pl.multiple_of(wrow + 128, 32), 32)], 14)

    small[0].wait()
    tokf = tok[...].astype(F32)
    ss = jnp.sum(tokf * tokf, axis=1, keepdims=True)
    e1s[...] = jnp.broadcast_to(ss, (ROWS, 128))

    small[1].wait()
    r0 = routes[0:1, :].astype(F32)
    r1 = routes[1:2, :].astype(F32)
    e_sub = iota((64, 64), 0).astype(F32)
    e_lane = iota((64, 64), 1).astype(F32)
    m0 = onehot(e_sub == r0)
    m1 = onehot(e_sub == r1)
    sub4 = iota((64, 256), 0)
    lane4 = iota((64, 256), 1) % 64
    same4 = onehot(sub4 == lane4)
    before4 = onehot(sub4 < lane4)
    n0 = jnp.sum(m0.astype(F32), axis=1, keepdims=True)
    a4 = nn(m0, same4) * (nn(m0, before4) + 1.0) + nn(m1, same4) * (nn(m1, before4) + n0 + 1.0)
    a4 = a4.astype(BF)

    def make_d(q, carry):
        row = iota((256, 1), 0)
        spread = onehot((row // 16 + q * 16) == iota((256, 64), 1))
        got = nn(spread, a4)
        hit = (got == ((row % 4) + 1).astype(F32)) & (((row // 4) % 4) == (iota((256, 256), 1) // 64))
        dmat[pl.ds(pl.multiple_of(q * 256, 256), 256), :] = onehot(hit)
        return carry

    lax.fori_loop(0, 4, make_d, 0)

    for k in (2, 3, 4):
        small[k].wait()
    step = jnp.exp(column(lgs[...], 64))
    mag = jnp.exp(-rate[...] * step)
    a_re = mag * jnp.cos(freq[...] * step)
    a_im = mag * jnp.sin(freq[...] * step)
    denom = rate[...] * rate[...] + freq[...] * freq[...]
    sh_re = a_re - 1.0
    fre[...] = (a_im * freq[...] - sh_re * rate[...]) / denom
    fim[...] = -(a_im * rate[...] + sh_re * freq[...]) / denom
    are[...] = a_re
    aim[...] = a_im
    l_imr.wait()
    l_imi.wait()

    def make_b(g, carry):
        rows = pl.ds(pl.multiple_of(g * 16, 16), 16)
        f_re = fre[pl.ds(g, 1), :]
        f_im = fim[pl.ds(g, 1), :]
        m_re = imr_v[rows, :]
        m_im = imi_v[rows, :]
        bre[rows, :] = (f_re * m_re - f_im * m_im).astype(BF)
        bim[rows, :] = (f_re * m_im + f_im * m_re).astype(BF)
        return carry

    lax.fori_loop(0, 64, make_b, 0)

    pl.semaphore_wait(barrier, greeted)

    def exchange(src, dst, k):
        c = pltpu.make_async_remote_copy(
            src_ref=src, dst_ref=dst, send_sem=e_send.at[k], recv_sem=e_recv.at[k],
            device_id=(ep, other), device_id_type=MESH,
        )
        c.start()
        return c

    x1 = exchange(e1s, e1r, 0)

    groups = [lax.rem(member + k, 8) for k in (6, 2, 5, 7, 1, 3, 4)]
    groups = [shard_of(colour, m) for m in groups]
    for piece in range(4):
        for dest in groups:
            for i, src in enumerate((sg, su)):
                pltpu.make_async_remote_copy(
                    src_ref=src.at[pl.ds(piece * 8, 8)],
                    dst_ref=wb.at[pl.ds(pl.multiple_of(wrow + i * 128 + piece * 8, 8), 8)],
                    send_sem=w_send, recv_sem=w_recv, device_id=(dest, tp), device_id_type=MESH,
                ).start()

    c0 = column(r0, 64)
    c1 = column(r1, 64)
    t0 = onehot(e_lane == c0)
    t1 = onehot(e_lane == c1)
    earlier = onehot(iota((64, 64), 1) < iota((64, 64), 0))
    b0 = (t0.astype(F32) * (nn(earlier, t0) + 1.0)).astype(BF)
    b1 = (t1.astype(F32) * (nn(earlier, t1) + jnp.sum(t0.astype(F32), axis=0, keepdims=True) + 1.0)).astype(BF)
    m0s[...] = t0.astype(F32)
    m1s[...] = t1.astype(F32)

    def make_dt(q, carry):
        lane = iota((1, 256), 1)
        spread = onehot((iota((64, 256), 0)) == (iota((64, 256), 1) // 16 + q * 16))
        want = ((lane % 4) + 1).astype(F32)
        cols = pl.ds(pl.multiple_of(q * 256, 256), 256)
        for route, coded in enumerate((b0, b1)):
            got = nn(coded, spread) == want
            for k in range(4):
                rows = pl.ds(route * 256 + k * 64, 64)
                dtmat[rows, cols] = onehot(got & (((lane // 4) % 4) == k))
        return carry

    lax.fori_loop(0, 4, make_dt, 0)
    pi = iota((256, 256), 0)
    pj = iota((256, 256), 1)
    perm[...] = onehot((((pi // 4) % 16) * 16 + (pi // 64) * 4 + pi % 4) == pj)
    permt[...] = onehot((((pi // 4) % 4) * 64 + (pi // 16) * 4 + pi % 4) == pj)
    small[7].wait()
    small[8].wait()
    rt[0:64, :] = erw[:, own_cols]
    rt[64:128, :] = jnp.concatenate([grw[:, own_cols].astype(F32), jnp.zeros((60, HALF), F32)], axis=0).astype(BF)

    x1.wait()
    small[5].wait()
    small[6].wait()
    total = ss + e1r[:, 0:1]
    scale = lax.rsqrt(total / WIDTH + EPS)
    vbuf[...] = (tokf * scale * mgain[:, own_cols]).astype(BF)
    l_omr.wait()
    l_omi.wait()
    cre[...] = omr_v[...].astype(BF)
    cim[...] = omi_v[...].astype(BF)
    l_sre.wait()
    l_sim.wait()
    lane_group = iota((ROWS, 128), 1) // 16

    def state_block(b, carry):
        cols = pl.ds(pl.multiple_of(b * 128, 128), 128)
        u = vbuf[:, cols]
        spread = jnp.concatenate([jnp.where(lane_group == j, u, jnp.zeros_like(u)) for j in range(8)], axis=0)
        d_re = nn(spread, bre[cols, :])
        d_im = nn(spread, bim[cols, :])
        fresh_re = []
        fresh_im = []
        for j in range(8):
            g = b * 8 + j
            at = pl.ds(g, ROWS, stride=PITCH)
            s_re = sre_v[at, :]
            s_im = sim_v[at, :]
            g_re = are[pl.ds(g, 1), :]
            g_im = aim[pl.ds(g, 1), :]
            n_re = g_re * s_re - g_im * s_im + d_re[j * ROWS:(j + 1) * ROWS]
            n_im = g_re * s_im + g_im * s_re + d_im[j * ROWS:(j + 1) * ROWS]
            sre_v[at, :] = n_re
            sim_v[at, :] = n_im
            fresh_re.append(n_re.astype(BF))
            fresh_im.append(n_im.astype(BF))
        read = nt(jnp.concatenate(fresh_re, axis=0), cre[cols, :]) - nt(jnp.concatenate(fresh_im, axis=0), cim[cols, :])
        mixed = skip[:, cols] * u.astype(F32)
        for j in range(8):
            mixed = mixed + jnp.where(lane_group == j, read[j * ROWS:(j + 1) * ROWS], 0.0)
        abuf[:, cols] = gelu(mixed).astype(BF)
        return carry

    lax.fori_loop(0, 8, state_block, 0)

    s_nre = load(kept_re, nre, 16)
    s_nim = load(kept_im, nim, 17)

    act = abuf[...]
    l_wv1.wait()
    vgs[0] = nn(act, wv_v[0]).astype(BF)
    x2 = exchange(vgs.at[0], vgr.at[0], 1)
    l_wg1.wait()
    vgs[1] = nn(act, wg_v[0]).astype(BF)
    x3 = exchange(vgs.at[1], vgr.at[1], 2)
    l_wv0.wait()
    value = nn(act, wv_v[1]).astype(BF).astype(F32)
    l_wg0.wait()
    gate = nn(act, wg_v[1]).astype(BF).astype(F32)
    x2.wait()
    x3.wait()
    value = value + vgr[0].astype(F32)
    gate = gate + vgr[1].astype(F32)
    mix = (value * sigmoid(gate)).astype(BF)
    hidden = (tok[...].astype(F32) + mix.astype(F32)).astype(BF).astype(F32)
    hid[...] = hidden
    small[9].wait()
    small[10].wait()
    scaled = hidden * egain[:, own_cols]
    top = scaled.astype(BF)
    rest = (scaled - top.astype(F32)).astype(BF)
    logits = nt(top, rt[...]) + nt(rest, rt[...])
    blend_part = jnp.sum(scaled * blend[:, own_cols], axis=1, keepdims=True)
    square_part = jnp.sum(hidden * hidden, axis=1, keepdims=True)
    lane = iota((ROWS, 128), 1)
    logits = jnp.where(lane == 68, blend_part, jnp.where(lane == 69, square_part, logits))
    e3s[...] = logits
    x4 = exchange(e3s, e3r, 3)
    x4.wait()
    logits = logits + e3r[...]
    squares = jnp.sum(jnp.where(lane == 69, logits, 0.0), axis=1, keepdims=True)
    inverse = lax.rsqrt(squares / WIDTH + EPS)
    hnorm = (scaled * inverse).astype(BF)
    logits = logits * inverse

    tb[0:ROWS, :] = hnorm
    quarters = jnp.concatenate([hnorm[:, k * 256:(k + 1) * 256] for k in range(4)], axis=0)
    dsend[...] = nn(dmat[...], quarters).astype(BF)
    mine = pl.ds(pl.multiple_of(ep * 16, 16), 16)
    xo[mine, :] = dsend[mine, :]

    def send_rows(src, dst, ssem, rsem):
        for dx, dy, dz in AROUND:
            dest = chip(dx, dy, dz)
            pltpu.make_async_remote_copy(
                src_ref=src.at[pl.ds(pl.multiple_of(dest * 16, 16), 16)], dst_ref=dst.at[mine],
                send_sem=ssem, recv_sem=rsem, device_id=(dest, tp), device_id_type=MESH,
            ).start()

    send_rows(dsend, xo, d_send, d_recv)
    tok_copies = []
    at = ROWS
    for i, (dx, dy, dz, first, rows) in enumerate(REACH):
        c = pltpu.make_async_remote_copy(
            src_ref=tb.at[pl.ds(first, rows)], dst_ref=tb.at[pl.ds(at, rows)],
            send_sem=t_send.at[i], recv_sem=t_recv.at[i], device_id=(chip(dx, dy, dz), tp), device_id_type=MESH,
        )
        c.start()
        tok_copies.append(c)
        at += rows

    def load_down(p, carry):
        i = shard_of(lax.div(p, 8), lax.rem(p, 8))
        pltpu.make_async_copy(
            sd.at[pl.ds(pl.multiple_of(i * 32, 32), 32)], sd_v.at[pl.ds(pl.multiple_of(p * 32, 32), 32)], lsem.at[15]
        ).start()
        return carry

    lax.fori_loop(0, 64, load_down, 0)

    blend_logit = jnp.sum(jnp.where(lane == 68, logits, 0.0), axis=1, keepdims=True)
    is_group = (lane >= 64) & (lane < 68)
    group_max = jnp.max(jnp.where(is_group, logits, -jnp.inf), axis=1, keepdims=True)
    group_exp = jnp.where(is_group, jnp.exp(jnp.where(is_group, logits, group_max) - group_max), 0.0)
    group_prob = group_exp / jnp.sum(group_exp, axis=1, keepdims=True)
    row0 = column(routes[0:1, :].astype(F32), 64).astype(I32)
    row1 = column(routes[1:2, :].astype(F32), 64).astype(I32)
    pick0 = jnp.sum(jnp.where(lane == row0, logits, 0.0), axis=1, keepdims=True)
    pick1 = jnp.sum(jnp.where(lane == row1, logits, 0.0), axis=1, keepdims=True)
    prob0 = jnp.sum(jnp.where(lane == 64 + row0 // 16, group_prob, 0.0), axis=1, keepdims=True)
    prob1 = jnp.sum(jnp.where(lane == 64 + row1 // 16, group_prob, 0.0), axis=1, keepdims=True)
    top_pick = jnp.maximum(pick0, pick1)
    exp0 = jnp.exp(pick0 - top_pick)
    exp1 = jnp.exp(pick1 - top_pick)
    weight0 = exp0 / (exp0 + exp1) * prob0
    weight1 = exp1 / (exp0 + exp1) * prob1
    blend_gate = sigmoid(blend_logit)

    bulk = pl.ds(0, (NEP - 1) * 16)
    pltpu.make_async_copy(xo.at[bulk], xo.at[bulk], d_recv).wait()
    x5 = exchange(xo, xp, 4)
    l_eg.wait()
    l_eu.wait()

    def unpack(src):
        for q in range(4):
            got = nn(perm[...], src[q * 256:(q + 1) * 256, :]).astype(BF)
            for k in range(4):
                xx[q * 64:(q + 1) * 64, k * 256:(k + 1) * 256] = got[k * 64:(k + 1) * 64]

    unpack(xo)
    acc[0] = nn(xx[...], eg_v[own_cols, :])
    acc[1] = nn(xx[...], eu_v[own_cols, :])
    x5.wait()
    unpack(xp)
    gate_e = acc[0] + nn(xx[...], eg_v[peer_cols, :])
    up_e = acc[1] + nn(xx[...], eu_v[peer_cols, :])
    inner[...] = (gate_e * sigmoid(gate_e) * up_e).astype(BF)
    l_ed.wait()
    pts[...] = nn(inner[...], ed_v[:, peer_cols]).astype(BF)
    x6 = exchange(pts, ptr, 5)
    part = nn(inner[...], ed_v[:, own_cols]).astype(BF)
    ptot[...] = part
    x6.wait()
    ptot[...] = (ptot[...].astype(F32) + ptr[...].astype(F32)).astype(BF)
    for q in range(4):
        rows = slice(q * 64, (q + 1) * 64)
        block = jnp.concatenate([ptot[rows, k * 256:(k + 1) * 256] for k in range(4)], axis=0)
        rsend[q * 256:(q + 1) * 256, :] = nn(permt[...], block).astype(BF)
    ret[mine, :] = rsend[mine, :]
    send_rows(rsend, ret, r_send, r_recv)

    l_sg.wait()
    l_su.wait()
    most = pl.ds(0, 7 * 64)
    pltpu.make_async_copy(wb.at[most], wb.at[most], w_recv).wait()
    for c in tok_copies:
        c.wait()
    peer_units = pl.ds(pl.multiple_of(other * 256, 256), 256)
    own_units = pl.ds(pl.multiple_of(tp * 256, 256), 256)
    dps[...] = nt(tb[...], wb[peer_units, :]).astype(BF)
    x7 = exchange(dps, dpr, 6)
    dense = nt(tb[...], wb[own_units, :]).astype(BF).astype(F32)
    x7.wait()
    dense = dense + dpr[...].astype(F32)
    dgate = dense[:, 0:128]
    dis[...] = (dgate * sigmoid(dgate) * dense[:, 128:256]).astype(BF)
    slot = pl.ds(pl.multiple_of((colour * 2 + tp) * ROWS, ROWS), ROWS)
    dn[slot, :] = dis[0:ROWS, :]

    def send_inner(at, first, rows, dest, core):
        base = (colour * 2 + tp) * ROWS + first
        pltpu.make_async_remote_copy(
            src_ref=dis.at[pl.ds(at, rows)], dst_ref=dn.at[pl.ds(pl.multiple_of(base, 32), rows)],
            send_sem=n_send, recv_sem=n_recv, device_id=(dest, core), device_id_type=MESH,
        ).start()

    at = ROWS
    for dx, dy, dz, first, rows in REACH:
        send_inner(at, first, rows, chip(-dx, -dy, -dz), tp)
        send_inner(at, first, rows, chip(-dx, -dy, -dz), other)
        at += rows
    send_inner(0, 0, ROWS, ep, other)
    pltpu.make_async_copy(ret.at[bulk], ret.at[bulk], r_recv).wait()
    got = nn(dtmat[...], ret[...])
    routed = [
        weight0 * got[k * 64:(k + 1) * 64] + weight1 * got[256 + k * 64:256 + (k + 1) * 64] for k in range(4)
    ]
    hid[...] = hid[...] + jnp.concatenate(routed, axis=1)

    pltpu.make_async_copy(sd, sd, lsem.at[15]).wait()
    fifteen = pl.ds(0, 15 * ROWS)
    pltpu.make_async_copy(dn.at[fifteen], dn.at[fifteen], n_recv).wait()
    dense_inner = jnp.concatenate([dn[s * ROWS:(s + 1) * ROWS, :] for s in range(16)], axis=1)
    out[...] = (hid[...] + blend_gate * nn(dense_inner, sd_v[...])).astype(BF)

    s_nre.wait()
    s_nim.wait()
    pltpu.make_async_copy(wb.at[most], wb.at[most], w_send).wait()
    pltpu.make_async_copy(xo.at[bulk], xo.at[bulk], d_send).wait()
    pltpu.make_async_copy(ret.at[bulk], ret.at[bulk], r_send).wait()
    pltpu.make_async_copy(dn.at[fifteen], dn.at[fifteen], n_send).wait()


def hand_out(result, next_re, next_im, out, nre, nim, out_v, re_v, im_v, sem):
    size = ROWS // PARTS
    moves = [(result, out_v, out)]
    for i in range(PARTS):
        rows = pl.ds(i * size, size)
        moves.append((next_re.at[rows], re_v.at[rows], nre.at[rows]))
        moves.append((next_im.at[rows], im_v.at[rows], nim.at[rows]))
    loads = [pltpu.make_async_copy(src, mid, sem.at[0, k]) for k, (src, mid, dst) in enumerate(moves)]
    stores = [pltpu.make_async_copy(mid, dst, sem.at[1, k]) for k, (src, mid, dst) in enumerate(moves)]
    for c in loads:
        c.start()
    for c, d in zip(loads, stores):
        c.wait()
        d.start()
    for d in stores:
        d.wait()


def shards(
    tokens, sequence_state_real, sequence_state_imaginary, mixer_norm_gain, expert_norm_gain, rate, freq,
    log_group_step, input_map_real, input_map_imaginary, output_map_real, output_map_imaginary, skip,
    mixer_value_weight, mixer_gate_weight, group_router_weight, expert_router_weight, dense_blend_weight, routes,
    expert_gate_weight, expert_up_weight, expert_down_weight, shared_gate_weight, shared_up_weight,
    shared_down_weight,
):
    vmem = pl.BlockSpec(memory_space=pltpu.VMEM)
    hbm = pl.BlockSpec(memory_space=pl.ANY)
    V = pltpu.VMEM
    D = pltpu.SemaphoreType.DMA
    state = jax.ShapeDtypeStruct((64, 64, 64), F32)
    operands = (
        tokens, mixer_norm_gain[None], expert_norm_gain[None], rate, freq, log_group_step[None], skip[None],
        group_router_weight.T, expert_router_weight.T, dense_blend_weight[None], routes.T,
        sequence_state_real, sequence_state_imaginary,
        jnp.swapaxes(input_map_real, 1, 2).reshape(1024, 64), jnp.swapaxes(input_map_imaginary, 1, 2).reshape(1024, 64),
        output_map_real.reshape(1024, 64), output_map_imaginary.reshape(1024, 64),
        mixer_value_weight, mixer_gate_weight, expert_gate_weight, expert_up_weight, expert_down_weight,
        shared_gate_weight.T, shared_up_weight.T, shared_down_weight,
    )
    scratch = [
        V((64, 1024), BF), V((1, 2048), F32), V((1, 2048), F32), V((64, 64), F32), V((64, 64), F32), V((1, 64), F32),
        V((1, 1024), F32), V((4, 2048), BF), V((64, 2048), BF), V((1, 2048), F32), V((2, 64), I32),
        V((64 * PITCH, 64), F32), V((64 * PITCH, 64), F32),
        V((1024, 64), F32), V((1024, 64), F32), V((1024, 64), F32), V((1024, 64), F32),
        V((2, 1024, 1024), BF), V((2, 1024, 1024), BF),
        V((2048, 512), BF), V((2048, 512), BF), V((512, 2048), BF),
        V((2048, 1024), BF), V((512, 1024), BF),
        V((64, 64), F32), V((64, 64), F32), V((64, 64), F32), V((64, 64), F32),
        V((1024, 64), BF), V((1024, 64), BF), V((1024, 64), BF), V((1024, 64), BF),
        V((64, 1024), BF), V((64, 1024), BF), V((128, 1024), BF),
        V((1024, 256), BF), V((512, 1024), BF), V((64, 64), F32), V((64, 64), F32), V((256, 256), BF), V((256, 256), BF),
        V((64, 128), F32), V((64, 128), F32), V((2, 64, 1024), BF), V((2, 64, 1024), BF),
        V((64, 128), F32), V((64, 128), F32),
        V((1024, 256), BF), V((1024, 256), BF), V((1024, 256), BF), V((256, 1024), BF),
        V((2, 256, 512), F32), V((256, 512), BF),
        V((256, 1024), BF), V((256, 1024), BF), V((256, 1024), BF),
        V((1024, 256), BF), V((1024, 256), BF),
        V((512, 1024), BF), V((512, 256), BF), V((512, 256), BF), V((512, 128), BF),
        V((1024, 128), BF), V((64, 1024), F32),
        D((29,)), D((7,)), D((7,)), D, D, D, D, D((len(REACH),)), D((len(REACH),)), D, D, D, D,
    ]
    result, next_re, next_im = pl.pallas_call(
        body,
        out_shape=(jax.ShapeDtypeStruct((64, 1024), BF), state, state),
        in_specs=[hbm] * 25,
        out_specs=(vmem, hbm, hbm),
        scratch_shapes=scratch,
        compiler_params=pltpu.CompilerParams(
            collective_id=0, has_side_effects=True, vmem_limit_bytes=60 * 1024 * 1024
        ),
    )(*operands)
    return pl.pallas_call(
        hand_out,
        out_shape=(jax.ShapeDtypeStruct((64, 1024), BF), state, state),
        in_specs=[hbm] * 3,
        out_specs=(hbm,) * 3,
        scratch_shapes=[V((64, 1024), BF), V((64, 64, 64), F32), V((64, 64, 64), F32), D((2, 2 * PARTS + 1))],
    )(result, next_re, next_im)


def solution(mesh):
    placed = (
        P("ep", "tp"),
        P("ep", "tp", None),
        P("ep", "tp", None),
        P(),
        P(),
        P("tp", None),
        P("tp", None),
        P("tp"),
        P("tp", None, None),
        P("tp", None, None),
        P("tp", None, None),
        P("tp", None, None),
        P("tp"),
        P("tp", None),
        P("tp", None),
        P(),
        P(),
        P(),
        P("ep", None),
        P("ep", None, "tp"),
        P("ep", None, "tp"),
        P("ep", "tp", None),
        P("tp", "ep"),
        P("tp", "ep"),
        P(None, "tp"),
    )
    return jax.shard_map(
        shards,
        mesh=mesh,
        in_specs=placed,
        out_specs=(P("ep", "tp"), P("ep", "tp", None), P("ep", "tp", None)),
        check_vma=False,
    )
```
